32 devices in a mesh: fs: 8 (over z, core), tp: 4 (over y, x).
Axes of the slice: x: 2, y: 2, z: 4, core: 2. Of those that a mesh axis runs over, the one named last changes fastest.
Arguments:
- rows_later: bfloat16 [6144, 2048], P('fs'), may hold values from -6 to 6
- rows_earlier: bfloat16 [6144, 2048], P('fs'), may hold values from -6 to 6
- out_cotangent: bfloat16 [6144, 4096], P('fs', 'tp'), may hold values from -6 to 6
- gate_proj: bfloat16 [2048, 4096], P('fs', 'tp'), may hold values from -0.125 to 0.125
- up_proj: bfloat16 [2048, 4096], P('fs', 'tp'), may hold values from -0.125 to 0.125
- conv_taps: float32 [3, 4096], P(None, 'tp'), may hold values from -4 to 4
- conv_bias: float32 [4096], P('tp'), may hold values from -3 to 3
- gate_grad_sum: float32 [2048, 4096], P('fs', 'tp'), may hold values from -6 to 6
- up_grad_sum: float32 [2048, 4096], P('fs', 'tp'), may hold values from -6 to 6
- taps_grad_sum: float32 [3, 4096], P(None, 'tp'), may hold values from -6 to 6
- bias_grad_sum: float32 [4096], P('tp'), may hold values from -6 to 6
Outputs:
- hidden_later: bfloat16 [6144, 4096], P('fs', 'tp')
- input_grad: bfloat16 [6144, 2048], P('fs')
- gate_grad_out: float32 [2048, 4096], P('fs', 'tp')
- up_grad_out: float32 [2048, 4096], P('fs', 'tp')
- taps_grad_out: float32 [3, 4096], P(None, 'tp')
- bias_grad_out: float32 [4096], P('tp')
The draws below stay inside these ranges and needn't reach their ends.
All inputs are finite; a program needn't handle non-finite values.
Results may differ from the reference program's by a relative error of at most 0.019.
Values may be sent and summed in bfloat16 or wider, within the bound.
A program may use at most 128 MiB of HBM per device.

```python
import jax
import jax.numpy as jnp
from jax import lax

D = 2048
FF = 4096
TAPS = 3
TOK_DEV = 768
TOKENS = 6144
N_FS = 8
N_TP = 4


def raised(result, rng, source, target, shards_of, factor):
    owner, partner = [(jnp.arange(result.shape[dim]) // (result.shape[dim] // shards_of)).reshape([-1 if axis == dim else 1 for axis in range(result.ndim)]) for dim in (source, target)]
    chosen = jax.random.permutation(rng, shards_of)[partner]
    strong = (owner == chosen) | (owner == (partner + shards_of // 2) % shards_of)
    return jnp.where(strong, factor * result, result)


def shard_levels(own_key, dims, pieces, low, top_value):
    loudness = 1.0
    for axis_at, shards_of in pieces:
        heights = jax.random.uniform(jax.random.fold_in(jax.random.fold_in(own_key, 6), axis_at), (shards_of,), jnp.float32, low / len(pieces), top_value / len(pieces))
        loudness = loudness * jnp.repeat(jnp.exp(heights), dims[axis_at] // shards_of).reshape((-1,) + (1,) * (len(dims) - 1 - axis_at))
    return loudness


def scatter_about(stream_key, dims, spread, limit, shards=(), kind=jnp.bfloat16):
    values = jax.random.normal(stream_key, dims, jnp.float32) * spread
    if len(shards) > 0:
        values = shard_levels(stream_key, dims, shards, -0.22, 0.18) * values
    return jnp.clip(values, min=-limit, max=limit).astype(kind)


def heavy_noise(own_key, shape, width, reach, pieces, heavy, dtype=jnp.bfloat16):
    result = width * jax.random.normal(own_key, shape, jnp.float32)
    if pieces:
        result = result * shard_levels(own_key, shape, pieces, -0.22, 0.18)
    return jnp.clip(raised(result, jax.random.fold_in(own_key, 3), *heavy), -reach, reach).astype(dtype)


def setup_inputs(seed: int = 0) -> dict:
    key_of = jax.random.split(jax.random.key(seed), 12)
    return {
        "rows_later": scatter_about(key_of[0], (TOKENS, D), 1.0, 6.0, ((0, 8),)),
        "rows_earlier": heavy_noise(key_of[1], (TOKENS, D), 1.0, 6.0, ((0, 8),), (0, 1, 8, 2.0)),
        "out_cotangent": heavy_noise(key_of[2], (TOKENS, FF), 1.0, 6.0, ((0, 8), (1, 4)), (0, 1, 8, 2.0)),
        "gate_proj": scatter_about(key_of[3], (D, FF), D ** -0.5, 0.125, ((0, 8), (1, 4))),
        "up_proj": scatter_about(key_of[4], (D, FF), D ** -0.5, 0.125, ((0, 8), (1, 4))),
        "conv_taps": scatter_about(key_of[5], (TAPS, FF), 0.6, 4.0, ((1, 4),), jnp.float32),
        "conv_bias": scatter_about(key_of[6], (FF,), 0.5, 3.0, ((0, 4),), jnp.float32),
        "gate_grad_sum": scatter_about(key_of[7], (D, FF), 1.0, 6.0, ((0, 8), (1, 4)), jnp.float32),
        "up_grad_sum": scatter_about(key_of[8], (D, FF), 1.0, 6.0, ((0, 8), (1, 4)), jnp.float32),
        "taps_grad_sum": scatter_about(key_of[9], (TAPS, FF), 1.0, 6.0, ((1, 4),), jnp.float32),
        "bias_grad_sum": scatter_about(key_of[10], (FF,), 1.0, 6.0, ((0, 4),), jnp.float32),
    }


def shift_down(values, distance):
    total_len = values.shape[1]
    return jnp.pad(values, ((0, 0), (distance, 0), (0, 0)))[:, :total_len]

def shift_up(values, distance):
    return jnp.pad(values, ((0, 0), (0, distance), (0, 0)))[:, distance:]

def causal_mix(pre_values, conv_taps, conv_bias):
    return conv_taps[0] * shift_down(pre_values, 2) + conv_taps[1] * shift_down(pre_values, 1) + conv_taps[2] * pre_values + conv_bias

def mix_adjoint(mixed_grad, conv_taps):
    return conv_taps[2] * mixed_grad + conv_taps[1] * shift_up(mixed_grad, 1) + conv_taps[0] * shift_up(mixed_grad, 2)

def reference(rows_later, rows_earlier, out_cotangent, gate_proj, up_proj, conv_taps, conv_bias, gate_grad_sum, up_grad_sum, taps_grad_sum, bias_grad_sum):
    stacked_rows = jnp.concatenate([rows_later, rows_earlier], axis=0)
    gate_pre = jnp.dot(stacked_rows, gate_proj, preferred_element_type=jnp.float32).astype(jnp.bfloat16)
    up_value = jnp.dot(stacked_rows, up_proj, preferred_element_type=jnp.float32).astype(jnp.bfloat16)
    gate_pre, up_value = lax.optimization_barrier((gate_pre, up_value))
    gate_float = gate_pre.astype(jnp.float32).reshape(2 * N_FS, TOK_DEV, FF)
    up_float = up_value.astype(jnp.float32).reshape(2 * N_FS, TOK_DEV, FF)
    mixed = causal_mix(gate_float, conv_taps, conv_bias)
    sig_all = jax.nn.sigmoid(mixed)
    activated = mixed * sig_all
    hidden = (activated * up_float).astype(jnp.bfloat16)
    hidden_later = hidden[:N_FS].reshape(TOKENS, FF)
    cotangent = out_cotangent.astype(jnp.float32).reshape(N_FS, TOK_DEV, FF)
    mixed_back = mixed[N_FS:]
    sig_back = sig_all[N_FS:]
    up_grad = (cotangent * activated[N_FS:]).astype(jnp.bfloat16).reshape(TOKENS, FF)
    mixed_grad = cotangent * up_float[N_FS:] * sig_back * (1.0 + mixed_back * (1.0 - sig_back))
    gate_grad = mix_adjoint(mixed_grad, conv_taps).astype(jnp.bfloat16).reshape(TOKENS, FF)
    block_width = FF // N_TP
    total = jnp.zeros((TOKENS, D), jnp.float32)
    for block_index in range(N_TP):
        column_start = block_index * block_width
        column_end = column_start + block_width
        part = jnp.dot(gate_grad[:, column_start:column_end], gate_proj[:, column_start:column_end].T, preferred_element_type=jnp.float32) + jnp.dot(up_grad[:, column_start:column_end], up_proj[:, column_start:column_end].T, preferred_element_type=jnp.float32)
        part = lax.optimization_barrier(part.astype(jnp.bfloat16))
        total = total + part.astype(jnp.float32)
    input_grad = total.astype(jnp.bfloat16)
    grad_scale = lax.rsqrt(jnp.asarray(TOKENS, jnp.float32))
    gate_grad_out = gate_grad_sum + grad_scale * jnp.dot(rows_earlier.T, gate_grad, preferred_element_type=jnp.float32)
    up_grad_out = up_grad_sum + grad_scale * jnp.dot(rows_earlier.T, up_grad, preferred_element_type=jnp.float32)
    gate_back = gate_float[N_FS:]
    tap_terms = jnp.stack([lax.optimization_barrier(jnp.sum(mixed_grad * shift_down(gate_back, 2 - tap_index), axis=(0, 1))) for tap_index in range(TAPS)])
    taps_grad_out = taps_grad_sum + grad_scale * tap_terms
    bias_grad_out = bias_grad_sum + grad_scale * lax.optimization_barrier(jnp.sum(mixed_grad, axis=(0, 1)))
    return (hidden_later, input_grad, gate_grad_out, up_grad_out, taps_grad_out, bias_grad_out)
```

```python
import functools
import math

import jax
import jax.numpy as jnp
from jax import lax
from jax.experimental import pallas as pl
from jax.experimental.pallas import tpu as pltpu
from jax.sharding import PartitionSpec as P

MESH = pl.DeviceIdType.MESH
VMEM_BYTES = 62 * 1024 * 1024
F32, BF16 = jnp.float32, jnp.bfloat16


def contract_last(left, right):
    return lax.dot_general(
        left, right, (((1,), (1,)), ((), ())), preferred_element_type=jnp.float32
    )


def down(values, distance):
    if distance == 0:
        return values
    index = lax.broadcasted_iota(jnp.int32, values.shape, 0)
    return jnp.where(index >= distance, pltpu.roll(values, distance, 0), 0.0)


def up(values, distance):
    if distance == 0:
        return values
    rows = values.shape[0]
    index = lax.broadcasted_iota(jnp.int32, values.shape, 0)
    return jnp.where(index < rows - distance, pltpu.roll(values, rows - distance, 0), 0.0)


class Sizes:
    def __init__(self, fs_size, tp_size, tokens, model, depth, width, taps):
        self.fs_size = fs_size
        self.chips = fs_size // 2
        self.side = math.isqrt(tp_size)
        self.tokens, self.model, self.depth, self.width = tokens, model, depth, width
        self.w = math.gcd(width, 128)
        self.n = width // self.w
        self.taps = taps
        block = tokens // (2 * self.side)
        self.q = max(q for q in (1, 2, 3, 4) if block % (16 * q) == 0)
        self.r = block // self.q
        self.scale = 1.0 / math.sqrt(tokens * fs_size)


def kernel(
    sizes,
    later_hbm,
    earlier_hbm,
    cot_hbm,
    gate_hbm,
    up_hbm,
    gate_sum_hbm,
    up_sum_hbm,
    taps_ref,
    bias_ref,
    taps_sum_ref,
    bias_sum_ref,
    hidden_hbm,
    rows_hbm,
    gate_out_hbm,
    up_out_hbm,
    taps_out,
    bias_out,
    later_v,
    earlier_v,
    earlier_t,
    cot_v,
    weights,
    pre,
    grads,
    hidden_v,
    acc,
    own_t,
    out_t,
    pair_t,
    ring,
    sums,
    rows_s,
    first_in,
    second_in,
    rows_buf,
    small_v,
    small_buf,
    weight_load,
    rows_load,
    cot_load,
    sum_load,
    sum_store,
    hidden_store,
    rows_store,
    line_send,
    line_recv,
    pair_send,
    pair_recv,
    term_send,
    term_recv,
    ring_send,
    ring_recv,
    first_send,
    first_recv,
    second_send,
    second_recv,
    third_send,
    third_recv,
    small_send,
    small_recv,
):
    n, w, q, r = sizes.n, sizes.w, sizes.q, sizes.r
    chips, side, depth = sizes.chips, sizes.side, sizes.depth
    fs_size, tokens, model = sizes.fs_size, sizes.tokens, sizes.model
    count = sizes.taps
    last = chips - 1
    fs = lax.axis_index("fs")
    tp = lax.axis_index("tp")
    z = fs // 2
    core = lax.rem(fs, 2)
    partner = 2 * z + 1 - core
    neighbours = (lax.rem(fs + 2, fs_size), lax.rem(fs + fs_size - 2, fs_size))
    ty = tp // side
    tx = lax.rem(tp, side)
    firsts = (tx, ty)
    seconds = (ty, tx)

    def first_peer(half, k):
        peer = lax.rem(firsts[half] + k, side)
        return peer, (ty * side + peer if half == 0 else peer * side + tx)

    def second_peer(half, k):
        peer = lax.rem(seconds[half] + k, side)
        return peer, (peer * side + tx if half == 0 else ty * side + peer)

    def columns(c):
        return pl.ds(pl.multiple_of(c * w, w), w)

    def own_rows(which):
        return pl.ds(pl.multiple_of((2 * z + which) * depth, depth), depth)

    def load_weight(c, which):
        source = (gate_hbm, up_hbm)[which]
        return pltpu.make_async_copy(
            source.at[:, columns(c)],
            weights.at[c, own_rows(core), pl.ds(which * w, w)],
            weight_load.at[c, which],
        )

    def load_rows(which):
        return pltpu.make_async_copy(
            (later_hbm, earlier_hbm)[which], (later_v, earlier_v)[which], rows_load.at[which]
        )

    def load_cot(c):
        return pltpu.make_async_copy(cot_hbm.at[:, columns(c)], cot_v.at[c], cot_load.at[c])

    def load_sum(c, which):
        source = (gate_sum_hbm, up_sum_hbm)[which]
        return pltpu.make_async_copy(
            source.at[:, columns(c)], sums.at[c, :, pl.ds(which * w, w)], sum_load.at[c, which]
        )

    def store_sum(c, which):
        target = (gate_out_hbm, up_out_hbm)[which]
        return pltpu.make_async_copy(
            sums.at[c, :, pl.ds(which * w, w)], target.at[:, columns(c)], sum_store.at[c, which]
        )

    def store_hidden(c):
        return pltpu.make_async_copy(
            hidden_v.at[c], hidden_hbm.at[:, columns(c)], hidden_store.at[c]
        )

    def piece(half, i, p):
        start = ((half * side + i) * q + p) * r
        return pl.ds(pl.multiple_of(start, r), r)

    def store_rows(half, i, p):
        block = piece(half, i, p)
        return pltpu.make_async_copy(
            rows_buf.at[block], rows_hbm.at[block], rows_store.at[half, i, p]
        )

    def remote(source, target, send, recv, device):
        return pltpu.make_async_remote_copy(
            src_ref=source,
            dst_ref=target,
            send_sem=send,
            recv_sem=recv,
            device_id=device,
            device_id_type=MESH,
        )

    def shard(o, which, c):
        return weights.at[c, pl.ds(pl.multiple_of((2 * o + which) * depth, depth), depth)]

    def line_copy(way, o, c):
        ref = shard(o, core, c)
        return remote(
            ref, ref, line_send.at[way, c, o], line_recv.at[c, o], {"fs": neighbours[way]}
        )

    def pair_copy(o, which, c):
        ref = shard(o, which, c)
        return remote(ref, ref, pair_send.at[c, o], pair_recv.at[c, o], {"fs": partner})

    def term_copy(c):
        return remote(
            out_t.at[lax.rem(c, 2)],
            pair_t.at[c],
            term_send.at[c],
            term_recv.at[c],
            {"fs": partner},
        )

    def ring_slot(way, c, d):
        return ring.at[way, c, d - 1 if way == 0 else d]

    def ring_copy(way, c, d):
        at = (way, c, d - 1 if way == 0 else d)
        slot = ring.at[at]
        return remote(slot, slot, ring_send.at[at], ring_recv.at[at], {"fs": neighbours[way]})

    def first_copy(half, k, p):
        peer, device = first_peer(half, k)
        at = (half, k - 1, p)
        return remote(
            rows_s.at[piece(half, peer, p)],
            first_in.at[at],
            first_send.at[at],
            first_recv.at[at],
            {"tp": device},
        )

    def second_copy(half, k, p, position):
        _, device = second_peer(half, k)
        slot = second_in.at[half, position, p]
        at = (half, k - 1, p)
        return remote(slot, slot, second_send.at[at], second_recv.at[at], {"tp": device})

    def third_copy(half, k, p, shown):
        _, device = first_peer(half, k)
        block = rows_buf.at[piece(half, shown, p)]
        at = (half, k - 1, p)
        return remote(block, block, third_send.at[at], third_recv.at[at], {"tp": device})

    def small_copy(k, slot):
        return remote(
            small_v,
            small_buf.at[slot],
            small_send.at[k - 1],
            small_recv.at[k - 1],
            {"fs": lax.rem(fs + k, fs_size)},
        )

    for c in range(n):
        load_weight(c, 0).start()
        load_weight(c, 1).start()

    barrier = pltpu.get_barrier_semaphore()
    for k in range(1, fs_size):
        pl.semaphore_signal(
            barrier, inc=1, device_id={"fs": lax.rem(fs + k, fs_size)}, device_id_type=MESH
        )
    for half in range(2):
        for k in range(1, side):
            pl.semaphore_signal(
                barrier, inc=1, device_id={"tp": first_peer(half, k)[1]}, device_id_type=MESH
            )

    load_rows(1).start()
    for c in range(n):
        load_cot(c).start()
    load_rows(0).start()
    for c in range(n):
        load_sum(c, 0).start()
        load_sum(c, 1).start()

    pl.semaphore_wait(barrier, fs_size - 1 + 2 * (side - 1))

    block = math.gcd(tokens, 256)
    wide = math.gcd(model, 512)

    def forward(rows_v, c):
        def body(index, carry):
            rows = pl.ds(pl.multiple_of(index * block, block), block)
            value = jnp.dot(rows_v[rows, :], weights[c], preferred_element_type=F32)
            pre[rows, :] = value.astype(BF16)
            return carry

        lax.fori_loop(0, tokens // block, body, 0)

    def mixing(c):
        gate = pre[:, :w].astype(F32)
        value = pre[:, w:].astype(F32)
        taps = [taps_ref[k : k + 1, columns(c)] for k in range(count)]
        shifted = [down(gate, count - 1 - k) for k in range(count)]
        mixed = bias_ref[:, columns(c)] + taps[0] * shifted[0]
        for k in range(1, count):
            mixed += taps[k] * shifted[k]
        sig = jax.nn.sigmoid(mixed)
        return value, taps, shifted, mixed, sig

    def middle_later(c):
        value, _, _, mixed, sig = mixing(c)
        hidden_v[c] = (mixed * sig * value).astype(BF16)

    def middle_earlier(c):
        value, taps, shifted, mixed, sig = mixing(c)
        cot = cot_v[c].astype(F32)
        grads[:, w:] = (cot * (mixed * sig)).astype(BF16)
        mixed_grad = cot * value * sig * (1.0 + mixed * (1.0 - sig))
        total = taps[count - 1] * mixed_grad
        for k in range(count - 1):
            total += taps[k] * up(mixed_grad, count - 1 - k)
        grads[:, :w] = total.astype(BF16)
        for k in range(count):
            small_v[c, k : k + 1, :] = jnp.sum(mixed_grad * shifted[k], axis=0, keepdims=True)
        small_v[c, count : count + 1, :] = jnp.sum(mixed_grad, axis=0, keepdims=True)

    def add_rows(c):
        def body(index, carry):
            cols = pl.ds(pl.multiple_of(index * wide, wide), wide)
            value = contract_last(grads[...], weights[c, cols, :])
            acc[:, cols] += value
            return carry

        lax.fori_loop(0, model // wide, body, 0)

    def last_rows(c):
        def body(index, carry):
            cols = pl.ds(pl.multiple_of(index * wide, wide), wide)
            value = contract_last(grads[...], weights[c, cols, :])
            rows_s[:, cols] = (acc[:, cols] + value).astype(BF16)
            return carry

        lax.fori_loop(0, model // wide, body, 0)
        for p in range(q):
            for k in range(1, side):
                for half in range(2):
                    first_copy(half, k, p).start()

    def make_terms(c):
        @pl.when(c >= 2)
        def _():
            term_copy(c - 2).wait_send()

        def fill(target, which):
            def body(d, carry):
                rows = pl.ds(pl.multiple_of((2 * d + which) * depth, depth), depth)
                value = jnp.dot(earlier_t[rows, :], grads[...], preferred_element_type=F32)
                target[d] = value.astype(BF16)
                return carry

            lax.fori_loop(0, chips, body, 0)

        fill(out_t.at[lax.rem(c, 2)], 1 - core)
        term_copy(c).start()
        fill(own_t.at[c], core)

    def transpose_rows():
        acc[...] = jnp.zeros_like(acc)
        small_v[...] = jnp.zeros_like(small_v)
        step = math.gcd(model, 256)

        def body(index, carry):
            cols = pl.ds(pl.multiple_of(index * step, step), step)
            earlier_t[cols, :] = earlier_v[:, cols].T
            return carry

        lax.fori_loop(0, model // step, body, 0)

    def compute(c):
        @pl.when(c == 0)
        def _():
            load_rows(1).wait()
            transpose_rows()

        for o in range(chips):
            pair_copy(o, 1 - core, c).wait_recv()
        forward(earlier_v, c)
        load_cot(c).wait()
        middle_earlier(c)

        @pl.when(c < n - 1)
        def _():
            add_rows(c)

        @pl.when(c == n - 1)
        def _():
            last_rows(c)
            for k in range(1, fs_size):
                small_copy(k, fs).start()

        make_terms(c)

        @pl.when(c == 0)
        def _():
            load_rows(0).wait()

        forward(later_v, c)
        middle_later(c)
        store_hidden(c).start()
        term_copy(c).wait_recv()

    def arrive(way, o, c, goes_on):
        line_copy(way, o, c).wait_recv()

        @pl.when(goes_on)
        def _():
            line_copy(way, o, c).start()

        pair_copy(o, core, c).start()

    def push(way, c, d, first_on_line):
        slot = ring_slot(way, c, d)

        @pl.when(first_on_line)
        def _():
            slot[...] = (own_t[c, d].astype(F32) + pair_t[c, d].astype(F32)).astype(BF16)

        @pl.when(jnp.logical_not(first_on_line))
        def _():
            ring_copy(way, c, d).wait_recv()
            total = own_t[c, d].astype(F32) + pair_t[c, d].astype(F32) + slot[...].astype(F32)
            slot[...] = total.astype(BF16)

        ring_copy(way, c, d).start()

    def push_up(c, carry):
        for d in range(last, 0, -1):

            @pl.when(d > z)
            def _():
                push(0, c, d, z == 0)

        return carry

    def push_down(c, carry):
        for d in range(last):

            @pl.when(d < z)
            def _():
                push(1, c, d, z == last)

        return carry

    def finish_sum(c, carry):
        load_sum(c, 0).wait()
        load_sum(c, 1).wait()
        base = own_t[c, z].astype(F32) + pair_t[c, z].astype(F32)
        sums[c] += sizes.scale * base

        @pl.when(z > 0)
        def _():
            ring_copy(0, c, z).wait_recv()
            sums[c] += sizes.scale * ring_slot(0, c, z)[...].astype(F32)

        @pl.when(z < last)
        def _():
            ring_copy(1, c, z).wait_recv()
            sums[c] += sizes.scale * ring_slot(1, c, z)[...].astype(F32)

        store_sum(c, 0).start()
        store_sum(c, 1).start()
        return carry

    far = jnp.maximum(z, last - z)
    lag = max(n // 2, 1)

    def pushed(i, hops):
        return jnp.clip(i + 1 - lag * hops + jnp.maximum(i - (n - 1), 0), 0, n)

    def exchange(j):
        for half in range(2):

            @pl.when(jnp.logical_and(j >= 1, j <= q))
            def _():
                p = j - 1
                total = rows_s[piece(half, firsts[half], p), :].astype(F32)
                for k in range(1, side):
                    first_copy(half, k, p).wait_recv()
                    total += first_in[half, k - 1, p].astype(F32)
                second_in[half, seconds[half], p] = total.astype(BF16)
                for k in range(1, side):
                    second_copy(half, k, p, seconds[half]).start()

            @pl.when(jnp.logical_and(j > q, j <= 2 * q))
            def _():
                p = j - 1 - q
                for k in range(1, side):
                    position = lax.rem(seconds[half] + side - k, side)
                    second_copy(half, k, p, position).wait_recv()
                total = second_in[half, 0, p].astype(F32)
                for position in range(1, side):
                    total += second_in[half, position, p].astype(F32)
                rows_buf[piece(half, firsts[half], p), :] = total.astype(BF16)
                for k in range(1, side):
                    third_copy(half, k, p, firsts[half]).start()
                store_rows(half, firsts[half], p).start()

            @pl.when(jnp.logical_and(j > 2 * q, j <= 3 * q))
            def _():
                p = j - 1 - 2 * q
                for k in range(1, side):
                    source = lax.rem(firsts[half] + side - k, side)
                    third_copy(half, k, p, source).wait_recv()
                    store_rows(half, source, p).start()

    def step(s, carry):
        i = s - far

        @pl.when(s < n)
        def _():
            load_weight(s, 0).wait()
            load_weight(s, 1).wait()

            @pl.when(z < last)
            def _():
                line_copy(0, z, s).start()

            @pl.when(z > 0)
            def _():
                line_copy(1, z, s).start()

            pair_copy(z, core, s).start()

        for k in range(1, chips):
            c = s - k
            inside = jnp.logical_and(c >= 0, c < n)

            @pl.when(jnp.logical_and(inside, z - k >= 0))
            def _():
                arrive(0, z - k, c, z < last)

            @pl.when(jnp.logical_and(inside, z + k <= last))
            def _():
                arrive(1, z + k, c, z > 0)

        @pl.when(jnp.logical_and(i >= 0, i < n))
        def _():
            compute(i)

        lax.fori_loop(pushed(i - 1, z), pushed(i, z), push_up, 0)
        lax.fori_loop(pushed(i - 1, last - z), pushed(i, last - z), push_down, 0)
        lax.fori_loop(pushed(i - 1, far), pushed(i, far), finish_sum, 0)
        exchange(i - (n - 1))
        return carry

    end = max(n - 1 + 3 * q, n - 1 + -(-lag * last // 2))
    lax.fori_loop(0, end + last + 1, step, 0)

    small_buf[fs] = small_v[...]
    for k in range(1, fs_size):
        small_copy(k, lax.rem(fs + fs_size - k, fs_size)).wait_recv()
    for c in range(n):
        total = small_buf[0, c]
        for source in range(1, fs_size):
            total += small_buf[source, c]
        total = sizes.scale * total
        cols = slice(c * w, (c + 1) * w)
        taps_out[:, cols] = taps_sum_ref[:, cols] + total[:count]
        bias_out[:, cols] = bias_sum_ref[:, cols] + total[count : count + 1]

    for k in range(1, fs_size):
        small_copy(k, fs).wait_send()

    def drain(c, carry):
        def over_chips(d, inner):
            pair_copy(d, core, c).wait_send()

            @pl.when(jnp.logical_and(d <= z, z < last))
            def _():
                line_copy(0, d, c).wait_send()

            @pl.when(jnp.logical_and(d >= z, z > 0))
            def _():
                line_copy(1, d, c).wait_send()

            @pl.when(d > z)
            def _():
                ring_copy(0, c, d).wait_send()

            @pl.when(d < z)
            def _():
                ring_copy(1, c, d).wait_send()

            return inner

        lax.fori_loop(0, chips, over_chips, 0)

        @pl.when(c >= n - 2)
        def _():
            term_copy(c).wait_send()

        store_hidden(c).wait()
        store_sum(c, 0).wait()
        store_sum(c, 1).wait()
        return carry

    lax.fori_loop(0, n, drain, 0)
    for half in range(2):
        for p in range(q):
            for k in range(1, side):
                first_copy(half, k, p).wait_send()
                second_copy(half, k, p, seconds[half]).wait_send()
                third_copy(half, k, p, firsts[half]).wait_send()
            for i in range(side):
                store_rows(half, i, p).wait()


def on_device(
    rows_later,
    rows_earlier,
    out_cotangent,
    gate_proj,
    up_proj,
    conv_taps,
    conv_bias,
    gate_grad_sum,
    up_grad_sum,
    taps_grad_sum,
    bias_grad_sum,
):
    tokens, model = rows_later.shape
    depth, width = gate_proj.shape
    taps = conv_taps.shape[0]
    sizes = Sizes(
        lax.axis_size("fs"), lax.axis_size("tp"), tokens, model, depth, width, taps
    )
    n, w, q, r = sizes.n, sizes.w, sizes.q, sizes.r
    chips, side, fs_size = sizes.chips, sizes.side, sizes.fs_size
    dma = pltpu.SemaphoreType.DMA
    whole = pl.BlockSpec(memory_space=pltpu.VMEM)
    far = pl.BlockSpec(memory_space=pl.ANY)
    links = max(side - 1, 1)
    outs = pl.pallas_call(
        functools.partial(kernel, sizes),
        out_shape=(
            jax.ShapeDtypeStruct((tokens, width), BF16),
            jax.ShapeDtypeStruct((tokens, model), BF16),
            jax.ShapeDtypeStruct((depth, width), F32),
            jax.ShapeDtypeStruct((depth, width), F32),
            jax.ShapeDtypeStruct((taps, width), F32),
            jax.ShapeDtypeStruct((1, width), F32),
        ),
        in_specs=[far] * 7 + [whole] * 4,
        out_specs=(far, far, far, far, whole, whole),
        scratch_shapes=[
            pltpu.VMEM((tokens, model), BF16),
            pltpu.VMEM((tokens, model), BF16),
            pltpu.VMEM((model, tokens), BF16),
            pltpu.VMEM((n, tokens, w), BF16),
            pltpu.VMEM((n, model, 2 * w), BF16),
            pltpu.VMEM((tokens, 2 * w), BF16),
            pltpu.VMEM((tokens, 2 * w), BF16),
            pltpu.VMEM((n, tokens, w), BF16),
            pltpu.VMEM((tokens, model), F32),
            pltpu.VMEM((n, chips, depth, 2 * w), BF16),
            pltpu.VMEM((2, chips, depth, 2 * w), BF16),
            pltpu.VMEM((n, chips, depth, 2 * w), BF16),
            pltpu.VMEM((2, n, max(chips - 1, 1), depth, 2 * w), BF16),
            pltpu.VMEM((n, depth, 2 * w), F32),
            pltpu.VMEM((tokens, model), BF16),
            pltpu.VMEM((2, links, q, r, model), BF16),
            pltpu.VMEM((2, side, q, r, model), BF16),
            pltpu.VMEM((tokens, model), BF16),
            pltpu.VMEM((n, 8 * -(-(taps + 1) // 8), w), F32),
            pltpu.VMEM((fs_size, n, 8 * -(-(taps + 1) // 8), w), F32),
            dma((n, 2)),
            dma((2,)),
            dma((n,)),
            dma((n, 2)),
            dma((n, 2)),
            dma((n,)),
            dma((2, side, q)),
            dma((2, n, chips)),
            dma((n, chips)),
            dma((n, chips)),
            dma((n, chips)),
            dma((n,)),
            dma((n,)),
            dma((2, n, max(chips - 1, 1))),
            dma((2, n, max(chips - 1, 1))),
        ]
        + [dma((2, links, q))] * 6
        + [dma((fs_size - 1,))] * 2,
        compiler_params=pltpu.CompilerParams(
            collective_id=0, has_side_effects=True, vmem_limit_bytes=VMEM_BYTES
        ),
    )(
        rows_later,
        rows_earlier,
        out_cotangent,
        gate_proj,
        up_proj,
        gate_grad_sum,
        up_grad_sum,
        conv_taps,
        conv_bias[None],
        taps_grad_sum,
        bias_grad_sum[None],
    )
    hidden_later, input_grad, gate_grad_out, up_grad_out, taps_grad_out, bias_grad_out = outs
    return (
        hidden_later,
        input_grad,
        gate_grad_out,
        up_grad_out,
        taps_grad_out,
        bias_grad_out[0],
    )


def solution(mesh):
    placed = (
        P("fs", None),
        P("fs", None),
        P("fs", "tp"),
        P("fs", "tp"),
        P("fs", "tp"),
        P(None, "tp"),
        P("tp"),
        P("fs", "tp"),
        P("fs", "tp"),
        P(None, "tp"),
        P("tp"),
    )
    return jax.shard_map(
        on_device,
        mesh=mesh,
        in_specs=placed,
        out_specs=(
            P("fs", "tp"),
            P("fs", None),
            P("fs", "tp"),
            P("fs", "tp"),
            P(None, "tp"),
            P("tp"),
        ),
        check_vma=False,
    )
```

```python
import functools
import math

import jax
import jax.numpy as jnp
from jax import lax
from jax.experimental import pallas as pl
from jax.experimental.pallas import tpu as pltpu
from jax.sharding import PartitionSpec as P

MESH = pl.DeviceIdType.MESH
VMEM_BYTES = 56 * 1024 * 1024
FORWARD_ROWS = 768
F32, BF16 = jnp.float32, jnp.bfloat16


def contract_last(left, right):
    return lax.dot_general(
        left, right, (((1,), (1,)), ((), ())), preferred_element_type=jnp.float32
    )


def down(values, distance):
    if distance == 0:
        return values
    index = lax.broadcasted_iota(jnp.int32, values.shape, 0)
    return jnp.where(index >= distance, pltpu.roll(values, distance, 0), 0.0)


def up(values, distance):
    if distance == 0:
        return values
    rows = values.shape[0]
    index = lax.broadcasted_iota(jnp.int32, values.shape, 0)
    return jnp.where(index < rows - distance, pltpu.roll(values, rows - distance, 0), 0.0)


class Sizes:
    def __init__(self, fs_size, tp_size, tokens, model, depth, width, taps):
        self.fs_size = fs_size
        self.chips = fs_size // 2
        self.side = math.isqrt(tp_size)
        self.tokens, self.model, self.depth, self.width = tokens, model, depth, width
        self.w = math.gcd(width, 128)
        self.n = width // self.w
        self.taps = taps
        self.group = math.gcd(self.n, 2)
        self.r = tokens // (2 * self.side)
        self.q = max(q for q in (1, 2, 4) if model % (128 * q) == 0)
        self.cut = model // self.q
        self.scale = 1.0 / math.sqrt(tokens * fs_size)


def kernel(
    sizes,
    later_hbm,
    earlier_hbm,
    cot_hbm,
    gate_hbm,
    up_hbm,
    gate_sum_hbm,
    up_sum_hbm,
    taps_ref,
    bias_ref,
    taps_sum_ref,
    bias_sum_ref,
    hidden_out,
    rows_out,
    gate_out,
    up_out,
    taps_out,
    bias_out,
    later_v,
    earlier_v,
    earlier_t,
    cot_v,
    weights,
    pre,
    grads,
    acc,
    own_t,
    out_t,
    pair_t,
    ring,
    rows_s,
    first_in,
    second_in,
    small_v,
    small_buf,
    weight_load,
    rows_load,
    cot_load,
    sum_load,
    line_send,
    line_recv,
    pair_send,
    pair_recv,
    term_send,
    term_recv,
    ring_send,
    ring_recv,
    first_send,
    first_recv,
    second_send,
    second_recv,
    third_send,
    third_recv,
    small_send,
    small_recv,
):
    n, w, q, r, cut = sizes.n, sizes.w, sizes.q, sizes.r, sizes.cut
    group = sizes.group
    chips, side, depth = sizes.chips, sizes.side, sizes.depth
    fs_size, tokens, model = sizes.fs_size, sizes.tokens, sizes.model
    count = sizes.taps
    last = chips - 1
    fs = lax.axis_index("fs")
    tp = lax.axis_index("tp")
    z = fs // 2
    core = lax.rem(fs, 2)
    partner = 2 * z + 1 - core
    neighbours = (lax.rem(fs + 2, fs_size), lax.rem(fs + fs_size - 2, fs_size))
    ty = tp // side
    tx = lax.rem(tp, side)
    firsts = (tx, ty)
    seconds = (ty, tx)

    def first_peer(half, k):
        peer = lax.rem(firsts[half] + k, side)
        return peer, (ty * side + peer if half == 0 else peer * side + tx)

    def second_peer(half, k):
        peer = lax.rem(seconds[half] + k, side)
        return peer, (peer * side + tx if half == 0 else ty * side + peer)

    def columns(c):
        return pl.ds(pl.multiple_of(c * w, w), w)

    def own_rows(which):
        return pl.ds(pl.multiple_of((2 * z + which) * depth, depth), depth)

    def load_weight(c, which):
        source = (gate_hbm, up_hbm)[which]
        return pltpu.make_async_copy(
            source.at[:, columns(c)],
            weights.at[c, own_rows(core), pl.ds(which * w, w)],
            weight_load.at[c, which],
        )

    def load_rows(which):
        return pltpu.make_async_copy(
            (later_hbm, earlier_hbm)[which], (later_v, earlier_v)[which], rows_load.at[which]
        )

    def load_cot(c):
        return pltpu.make_async_copy(cot_hbm.at[:, columns(c)], cot_v.at[c], cot_load.at[c])

    def load_sum(which):
        return pltpu.make_async_copy(
            (gate_sum_hbm, up_sum_hbm)[which], (gate_out, up_out)[which], sum_load.at[which]
        )

    def piece(half, i, p):
        rows = pl.ds(pl.multiple_of((half * side + i) * r, r), r)
        return rows, pl.ds(pl.multiple_of(p * cut, cut), cut)

    def remote(source, target, send, recv, device):
        return pltpu.make_async_remote_copy(
            src_ref=source,
            dst_ref=target,
            send_sem=send,
            recv_sem=recv,
            device_id=device,
            device_id_type=MESH,
        )

    def shard(o, which, c):
        return weights.at[c, pl.ds(pl.multiple_of((2 * o + which) * depth, depth), depth)]

    def line_copy(way, o, c):
        ref = shard(o, core, c)
        return remote(
            ref, ref, line_send.at[way, c, o], line_recv.at[c, o], {"fs": neighbours[way]}
        )

    def pair_copy(o, which, c):
        ref = shard(o, which, c)
        return remote(ref, ref, pair_send.at[c, o], pair_recv.at[c, o], {"fs": partner})

    def term_copy(c):
        return remote(
            out_t.at[lax.rem(c, 2)],
            pair_t.at[c],
            term_send.at[c],
            term_recv.at[c],
            {"fs": partner},
        )

    def ring_slot(way, c, d):
        return ring.at[way, c, d - 1 if way == 0 else d]

    def ring_copy(way, c, d):
        at = (way, c, d - 1 if way == 0 else d)
        slot = ring.at[at]
        return remote(slot, slot, ring_send.at[at], ring_recv.at[at], {"fs": neighbours[way]})

    def first_copy(half, k, p):
        peer, device = first_peer(half, k)
        at = (half, k - 1, p)
        return remote(
            rows_s.at[piece(half, peer, p)],
            first_in.at[at],
            first_send.at[at],
            first_recv.at[at],
            {"tp": device},
        )

    def second_copy(half, k, p, position):
        _, device = second_peer(half, k)
        slot = second_in.at[half, position, p]
        at = (half, k - 1, p)
        return remote(slot, slot, second_send.at[at], second_recv.at[at], {"tp": device})

    def third_copy(half, k, p, shown):
        _, device = first_peer(half, k)
        block = rows_out.at[piece(half, shown, p)]
        at = (half, k - 1, p)
        return remote(block, block, third_send.at[at], third_recv.at[at], {"tp": device})

    def small_copy(k, slot):
        return remote(
            small_v,
            small_buf.at[slot],
            small_send.at[k - 1],
            small_recv.at[k - 1],
            {"fs": lax.rem(fs + k, fs_size)},
        )

    for c in range(n):
        load_weight(c, 0).start()
        load_weight(c, 1).start()

    barrier = pltpu.get_barrier_semaphore()
    for k in range(1, fs_size):
        pl.semaphore_signal(
            barrier, inc=1, device_id={"fs": lax.rem(fs + k, fs_size)}, device_id_type=MESH
        )
    for half in range(2):
        for k in range(1, side):
            pl.semaphore_signal(
                barrier, inc=1, device_id={"tp": first_peer(half, k)[1]}, device_id_type=MESH
            )

    load_rows(1).start()
    for c in range(n):
        load_cot(c).start()
    load_rows(0).start()
    load_sum(0).start()
    load_sum(1).start()

    pl.semaphore_wait(barrier, fs_size - 1 + 2 * (side - 1))

    block = math.gcd(tokens, FORWARD_ROWS)

    def forward(rows_v, c):
        def body(index, carry):
            rows = pl.ds(pl.multiple_of(index * block, block), block)
            value = jnp.dot(rows_v[rows, :], weights[c], preferred_element_type=F32)
            pre[rows, :] = value.astype(BF16)
            return carry

        lax.fori_loop(0, tokens // block, body, 0)

    def mixing(c):
        gate = pre[:, :w].astype(F32)
        value = pre[:, w:].astype(F32)
        taps = [taps_ref[k : k + 1, columns(c)] for k in range(count)]
        shifted = [down(gate, count - 1 - k) for k in range(count)]
        mixed = bias_ref[:, columns(c)] + taps[0] * shifted[0]
        for k in range(1, count):
            mixed += taps[k] * shifted[k]
        sig = jax.nn.sigmoid(mixed)
        return value, taps, shifted, mixed, sig

    def middle_later(c):
        value, _, _, mixed, sig = mixing(c)
        hidden_out[:, columns(c)] = (mixed * sig * value).astype(BF16)

    def middle_earlier(c):
        value, taps, shifted, mixed, sig = mixing(c)
        cot = cot_v[c].astype(F32)
        grads[c, :, w:] = (cot * (mixed * sig)).astype(BF16)
        mixed_grad = cot * value * sig * (1.0 + mixed * (1.0 - sig))
        total = taps[count - 1] * mixed_grad
        for k in range(count - 1):
            total += taps[k] * up(mixed_grad, count - 1 - k)
        grads[c, :, :w] = total.astype(BF16)
        for k in range(count):
            small_v[c, k : k + 1, :] = jnp.sum(mixed_grad * shifted[k], axis=0, keepdims=True)
        small_v[c, count : count + 1, :] = jnp.sum(mixed_grad, axis=0, keepdims=True)

    def rows_part(c, cols):
        value = contract_last(grads[c - group + 1], weights[c - group + 1, cols, :])
        for k in range(1, group):
            at = c - group + 1 + k
            value += contract_last(grads[at], weights[at, cols, :])
        return value

    def add_rows(c):
        def body(p, carry):
            cols = pl.ds(pl.multiple_of(p * cut, cut), cut)
            acc[:, cols] += rows_part(c, cols)
            return carry

        lax.fori_loop(0, q, body, 0)

    def last_rows(c):
        def body(p, carry):
            cols = pl.ds(pl.multiple_of(p * cut, cut), cut)
            rows_s[:, cols] = (acc[:, cols] + rows_part(c, cols)).astype(BF16)
            for k in range(1, side):
                for half in range(2):
                    first_copy(half, k, p).start()
            return carry

        lax.fori_loop(0, q, body, 0)

    def make_terms(c, carry):
        slot = lax.rem(c, 2)

        @pl.when(c >= 2)
        def _():
            term_copy(c - 2).wait_send()

        half_rows = chips * depth
        value = jnp.dot(earlier_t[...], grads[c], preferred_element_type=F32)
        out_t[slot] = value[:half_rows].astype(BF16)
        own_t[c] = value[half_rows:].astype(BF16)
        term_copy(c).start()
        return carry

    def wait_terms(c, carry):
        term_copy(c).wait_recv()
        return carry

    def transpose_rows():
        acc[...] = jnp.zeros_like(acc)
        small_v[...] = jnp.zeros_like(small_v)

        def body(d, carry):
            cols = pl.ds(pl.multiple_of(d * 2 * depth, 2 * depth), 2 * depth)
            value = earlier_v[:, cols].T
            for which in range(2):
                owner = jnp.where(core == which, chips + d, d)
                rows = pl.ds(pl.multiple_of(owner * depth, depth), depth)
                earlier_t[rows, :] = value[which * depth : (which + 1) * depth]
            return carry

        lax.fori_loop(0, chips, body, 0)

    def compute_first(c):
        @pl.when(c == 0)
        def _():
            load_rows(1).wait()
            load_sum(0).wait()
            load_sum(1).wait()
            transpose_rows()

        for o in range(chips):
            pair_copy(o, 1 - core, c).wait_recv()
        forward(earlier_v, c)

    def compute_second(c):
        load_cot(c).wait()
        middle_earlier(c)

        @pl.when(jnp.logical_and(c < n - 1, lax.rem(c, group) == group - 1))
        def _():
            add_rows(c)

        @pl.when(c == n - 1)
        def _():
            last_rows(c)
            for k in range(1, fs_size):
                small_copy(k, fs).start()

    def compute_later(c):
        @pl.when(c == 0)
        def _():
            load_rows(0).wait()

        forward(later_v, c)
        middle_later(c)

    def arrive(way, o, c, goes_on):
        line_copy(way, o, c).wait_recv()

        @pl.when(goes_on)
        def _():
            line_copy(way, o, c).start()

        pair_copy(o, core, c).start()

    def terms_of(c, d):
        rows = pl.ds(pl.multiple_of(d * depth, depth), depth)
        return own_t[c, rows, :].astype(F32) + pair_t[c, rows, :].astype(F32)

    def push(way, c, d, first_on_line):
        slot = ring_slot(way, c, d)

        @pl.when(first_on_line)
        def _():
            slot[...] = terms_of(c, d).astype(BF16)

        @pl.when(jnp.logical_not(first_on_line))
        def _():
            ring_copy(way, c, d).wait_recv()
            slot[...] = (terms_of(c, d) + slot[...].astype(F32)).astype(BF16)

        ring_copy(way, c, d).start()

    def push_up(c, carry):
        for d in range(last, 0, -1):

            @pl.when(d > z)
            def _():
                push(0, c, d, z == 0)

        return carry

    def push_down(c, carry):
        for d in range(last):

            @pl.when(d < z)
            def _():
                push(1, c, d, z == last)

        return carry

    def finish_sum(c, carry):
        def add(value):
            gate_out[:, columns(c)] += sizes.scale * value[:, :w]
            up_out[:, columns(c)] += sizes.scale * value[:, w:]

        base = terms_of(c, z)

        @pl.when(z == 0)
        def _():
            ring_copy(1, c, z).wait_recv()
            add(base + ring_slot(1, c, z)[...].astype(F32))

        @pl.when(z == last)
        def _():
            ring_copy(0, c, z).wait_recv()
            add(base + ring_slot(0, c, z)[...].astype(F32))

        @pl.when(jnp.logical_and(z > 0, z < last))
        def _():
            ring_copy(0, c, z).wait_recv()
            ring_copy(1, c, z).wait_recv()
            add(
                base
                + ring_slot(0, c, z)[...].astype(F32)
                + ring_slot(1, c, z)[...].astype(F32)
            )

        return carry

    far = jnp.maximum(z, last - z)

    def termed(i):
        return jnp.where(i >= n, n, jnp.clip(i, 0, max(n - 2, 0)))

    def pushed(i, hops):
        turn = i - (n - 1) - 2 * (hops - 1)
        after = jnp.where(turn >= 1, jnp.clip(3 + (turn - 1) // 2, 0, n), 0)
        return jnp.where(hops == 0, termed(i), after)

    def exchange(j):
        for half in range(2):

            @pl.when(jnp.logical_and(j >= 1, j <= q))
            def _():
                p = j - 1
                total = rows_s[piece(half, firsts[half], p)].astype(F32)
                for k in range(1, side):
                    first_copy(half, k, p).wait_recv()
                    total += first_in[half, k - 1, p].astype(F32)
                second_in[half, seconds[half], p] = total.astype(BF16)
                for k in range(1, side):
                    second_copy(half, k, p, seconds[half]).start()

            @pl.when(jnp.logical_and(j > q, j <= 2 * q))
            def _():
                p = j - 1 - q
                for k in range(1, side):
                    position = lax.rem(seconds[half] + side - k, side)
                    second_copy(half, k, p, position).wait_recv()
                total = second_in[half, 0, p].astype(F32)
                for position in range(1, side):
                    total += second_in[half, position, p].astype(F32)
                rows_out[piece(half, firsts[half], p)] = total.astype(BF16)
                for k in range(1, side):
                    third_copy(half, k, p, firsts[half]).start()

            @pl.when(jnp.logical_and(j > 2 * q, j <= 3 * q))
            def _():
                p = j - 1 - 2 * q
                for k in range(1, side):
                    source = lax.rem(firsts[half] + side - k, side)
                    third_copy(half, k, p, source).wait_recv()

    at_end = jnp.logical_or(z == 0, z == last)

    def send_own(c, carry):
        load_weight(c, 0).wait()
        load_weight(c, 1).wait()

        @pl.when(z < last)
        def _():
            line_copy(0, z, c).start()

        @pl.when(z > 0)
        def _():
            line_copy(1, z, c).start()

        pair_copy(z, core, c).start()
        return carry

    @pl.when(at_end)
    def _():
        lax.fori_loop(0, n, send_own, 0)

    def step(s, carry):
        i = s - far

        @pl.when(jnp.logical_and(s < n, jnp.logical_not(at_end)))
        def _():
            send_own(s, 0)

        for k in range(1, chips):
            c = s - k
            inside = jnp.logical_and(c >= 0, c < n)

            @pl.when(jnp.logical_and(inside, z - k >= 0))
            def _():
                arrive(0, z - k, c, z < last)

            @pl.when(jnp.logical_and(inside, z + k <= last))
            def _():
                arrive(1, z + k, c, z > 0)

        lax.fori_loop(termed(i - 1), termed(i), make_terms, 0)

        @pl.when(jnp.logical_and(i >= 0, i < n))
        def _():
            compute_first(i)

        exchange(i - (n - 1))
        lax.fori_loop(termed(i - 1), termed(i), wait_terms, 0)
        lax.fori_loop(pushed(i - 1, z), pushed(i, z), push_up, 0)
        lax.fori_loop(pushed(i - 1, last - z), pushed(i, last - z), push_down, 0)
        hops = jnp.where(at_end, 1, far)
        lax.fori_loop(pushed(i - 1, hops), pushed(i, hops), finish_sum, 0)

        @pl.when(jnp.logical_and(i >= 0, i < n))
        def _():
            compute_second(i)

        @pl.when(jnp.logical_and(i >= n, i < 2 * n))
        def _():
            compute_later(i - n)

        return carry

    turns = 2 * max(n - 3, 0) + 1 + 2 * max(last - 2, 0)
    end = n - 1 + max(3 * q, n, turns)
    lax.fori_loop(0, end + last + 1, step, 0)

    small_buf[fs] = small_v[...]
    for k in range(1, fs_size):
        small_copy(k, lax.rem(fs + fs_size - k, fs_size)).wait_recv()
    for c in range(n):
        total = small_buf[0, c]
        for source in range(1, fs_size):
            total += small_buf[source, c]
        total = sizes.scale * total
        cols = slice(c * w, (c + 1) * w)
        taps_out[:, cols] = taps_sum_ref[:, cols] + total[:count]
        bias_out[:, cols] = bias_sum_ref[:, cols] + total[count : count + 1]

    for k in range(1, fs_size):
        small_copy(k, fs).wait_send()

    def drain(c, carry):
        def over_chips(d, inner):
            pair_copy(d, core, c).wait_send()

            @pl.when(jnp.logical_and(d <= z, z < last))
            def _():
                line_copy(0, d, c).wait_send()

            @pl.when(jnp.logical_and(d >= z, z > 0))
            def _():
                line_copy(1, d, c).wait_send()

            @pl.when(d > z)
            def _():
                ring_copy(0, c, d).wait_send()

            @pl.when(d < z)
            def _():
                ring_copy(1, c, d).wait_send()

            return inner

        lax.fori_loop(0, chips, over_chips, 0)

        @pl.when(c >= n - 2)
        def _():
            term_copy(c).wait_send()

        return carry

    lax.fori_loop(0, n, drain, 0)
    for half in range(2):
        for p in range(q):
            for k in range(1, side):
                first_copy(half, k, p).wait_send()
                second_copy(half, k, p, seconds[half]).wait_send()
                third_copy(half, k, p, firsts[half]).wait_send()


def store_kernel(*refs):
    count = len(refs) // 2
    sources, targets, sems = refs[:count], refs[count : 2 * count], refs[-1]
    copies = [
        pltpu.make_async_copy(sources[at], targets[at], sems.at[at]) for at in range(count)
    ]
    for copy in copies:
        copy.start()
    for copy in copies:
        copy.wait()


def on_device(
    rows_later,
    rows_earlier,
    out_cotangent,
    gate_proj,
    up_proj,
    conv_taps,
    conv_bias,
    gate_grad_sum,
    up_grad_sum,
    taps_grad_sum,
    bias_grad_sum,
):
    tokens, model = rows_later.shape
    depth, width = gate_proj.shape
    taps = conv_taps.shape[0]
    sizes = Sizes(
        lax.axis_size("fs"), lax.axis_size("tp"), tokens, model, depth, width, taps
    )
    n, w, q, r, cut = sizes.n, sizes.w, sizes.q, sizes.r, sizes.cut
    chips, side, fs_size = sizes.chips, sizes.side, sizes.fs_size
    dma = pltpu.SemaphoreType.DMA
    whole = pl.BlockSpec(memory_space=pltpu.VMEM)
    far = pl.BlockSpec(memory_space=pl.ANY)
    links = max(side - 1, 1)
    outs = pl.pallas_call(
        functools.partial(kernel, sizes),
        out_shape=(
            pltpu.VMEM((tokens, width), BF16),
            pltpu.VMEM((tokens, model), BF16),
            pltpu.VMEM((depth, width), F32),
            pltpu.VMEM((depth, width), F32),
            pltpu.VMEM((taps, width), F32),
            pltpu.VMEM((1, width), F32),
        ),
        in_specs=[far] * 7 + [whole] * 4,
        out_specs=(whole,) * 6,
        scratch_shapes=[
            pltpu.VMEM((tokens, model), BF16),
            pltpu.VMEM((tokens, model), BF16),
            pltpu.VMEM((model, tokens), BF16),
            pltpu.VMEM((n, tokens, w), BF16),
            pltpu.VMEM((n, model, 2 * w), BF16),
            pltpu.VMEM((tokens, 2 * w), BF16),
            pltpu.VMEM((n, tokens, 2 * w), BF16),
            pltpu.VMEM((tokens, model), F32),
            pltpu.VMEM((n, chips * depth, 2 * w), BF16),
            pltpu.VMEM((2, chips * depth, 2 * w), BF16),
            pltpu.VMEM((n, chips * depth, 2 * w), BF16),
            pltpu.VMEM((2, n, max(chips - 1, 1), depth, 2 * w), BF16),
            pltpu.VMEM((tokens, model), BF16),
            pltpu.VMEM((2, links, q, r, cut), BF16),
            pltpu.VMEM((2, side, q, r, cut), BF16),
            pltpu.VMEM((n, 8 * -(-(taps + 1) // 8), w), F32),
            pltpu.VMEM((fs_size, n, 8 * -(-(taps + 1) // 8), w), F32),
            dma((n, 2)),
            dma((2,)),
            dma((n,)),
            dma((2,)),
            dma((2, n, chips)),
            dma((n, chips)),
            dma((n, chips)),
            dma((n, chips)),
            dma((n,)),
            dma((n,)),
            dma((2, n, max(chips - 1, 1))),
            dma((2, n, max(chips - 1, 1))),
        ]
        + [dma((2, links, q))] * 6
        + [dma((fs_size - 1,))] * 2,
        compiler_params=pltpu.CompilerParams(
            collective_id=0, has_side_effects=True, vmem_limit_bytes=VMEM_BYTES
        ),
    )(
        rows_later,
        rows_earlier,
        out_cotangent,
        gate_proj,
        up_proj,
        gate_grad_sum,
        up_grad_sum,
        conv_taps,
        conv_bias[None],
        taps_grad_sum,
        bias_grad_sum[None],
    )
    stored = pl.pallas_call(
        store_kernel,
        out_shape=tuple(jax.ShapeDtypeStruct(out.shape, out.dtype) for out in outs),
        in_specs=[whole] * len(outs),
        out_specs=(far,) * len(outs),
        scratch_shapes=[dma((len(outs),))],
        compiler_params=pltpu.CompilerParams(vmem_limit_bytes=1024 * 1024),
    )(*[pltpu.with_memory_space_constraint(out, pltpu.VMEM) for out in outs])
    return stored[:5] + (stored[5][0],)


def solution(mesh):
    placed = (
        P("fs", None),
        P("fs", None),
        P("fs", "tp"),
        P("fs", "tp"),
        P("fs", "tp"),
        P(None, "tp"),
        P("tp"),
        P("fs", "tp"),
        P("fs", "tp"),
        P(None, "tp"),
        P("tp"),
    )
    return jax.shard_map(
        on_device,
        mesh=mesh,
        in_specs=placed,
        out_specs=(
            P("fs", "tp"),
            P("fs", None),
            P("fs", "tp"),
            P("fs", "tp"),
            P(None, "tp"),
            P("tp"),
        ),
        check_vma=False,
    )
```

```python
import functools
import math

import jax
import jax.numpy as jnp
from jax import lax
from jax.experimental import pallas as pl
from jax.experimental.pallas import tpu as pltpu
from jax.sharding import PartitionSpec as P

MESH = pl.DeviceIdType.MESH
VMEM_BYTES = 57 * 1024 * 1024
FORWARD_ROWS = 768
F32, BF16 = jnp.float32, jnp.bfloat16


def contract_last(left, right):
    return lax.dot_general(
        left, right, (((1,), (1,)), ((), ())), preferred_element_type=jnp.float32
    )


def down(values, distance):
    if distance == 0:
        return values
    index = lax.broadcasted_iota(jnp.int32, values.shape, 0)
    return jnp.where(index >= distance, pltpu.roll(values, distance, 0), 0.0)


def up(values, distance):
    if distance == 0:
        return values
    rows = values.shape[0]
    index = lax.broadcasted_iota(jnp.int32, values.shape, 0)
    return jnp.where(index < rows - distance, pltpu.roll(values, rows - distance, 0), 0.0)


class Sizes:
    def __init__(self, fs_size, tp_size, tokens, model, depth, width, taps):
        self.fs_size = fs_size
        self.chips = fs_size // 2
        self.side = math.isqrt(tp_size)
        self.tokens, self.model, self.depth, self.width = tokens, model, depth, width
        self.w = math.gcd(width, 128)
        self.n = width // self.w
        self.taps = taps
        self.group = math.gcd(self.n, 2)
        self.tail = min(self.n, 2 * self.group)
        self.r = tokens // (2 * self.side)
        self.q = max(q for q in (1, 2, 4, 8) if model % (128 * q) == 0)
        self.cut = model // self.q
        self.scale = 1.0 / math.sqrt(tokens * fs_size)


def kernel(
    sizes,
    later_hbm,
    earlier_hbm,
    cot_hbm,
    gate_hbm,
    up_hbm,
    gate_sum_hbm,
    up_sum_hbm,
    taps_hbm,
    bias_hbm,
    taps_sum_hbm,
    bias_sum_hbm,
    hidden_out,
    rows_out,
    gate_out,
    up_out,
    taps_out,
    bias_out,
    later_v,
    earlier_v,
    earlier_t,
    cot_v,
    weights,
    pre,
    grads,
    acc,
    own_t,
    out_t,
    pair_t,
    ring,
    rows_s,
    help_in,
    help_out,
    help_send,
    help_recv,
    back_send,
    back_recv,
    first_in,
    second_in,
    small_v,
    small_in,
    small_buf,
    taps_ref,
    bias_ref,
    taps_sum_ref,
    bias_sum_ref,
    mix_load,
    weight_load,
    rows_load,
    cot_load,
    sum_load,
    line_send,
    line_recv,
    pair_send,
    pair_recv,
    term_send,
    term_recv,
    ring_send,
    ring_recv,
    first_send,
    first_recv,
    second_send,
    second_recv,
    third_send,
    third_recv,
    small_send,
    small_recv,
):
    n, w, q, r, cut = sizes.n, sizes.w, sizes.q, sizes.r, sizes.cut
    group, tail = sizes.group, sizes.tail
    chips, side, depth = sizes.chips, sizes.side, sizes.depth
    fs_size, tokens, model = sizes.fs_size, sizes.tokens, sizes.model
    count = sizes.taps
    last = chips - 1
    fs = lax.axis_index("fs")
    tp = lax.axis_index("tp")
    z = fs // 2
    core = lax.rem(fs, 2)
    partner = 2 * z + 1 - core
    at_end = jnp.logical_or(z == 0, z == last)
    helped = chips >= 4
    helper = jnp.logical_and(helped, jnp.logical_or(z == 1, z == last - 1))
    neighbours = (lax.rem(fs + 2, fs_size), lax.rem(fs + fs_size - 2, fs_size))
    ty = tp // side
    tx = lax.rem(tp, side)
    firsts = (tx, ty)
    seconds = (ty, tx)

    def first_peer(half, k):
        peer = lax.rem(firsts[half] + k, side)
        return peer, (ty * side + peer if half == 0 else peer * side + tx)

    def second_peer(half, k):
        peer = lax.rem(seconds[half] + k, side)
        return peer, (peer * side + tx if half == 0 else ty * side + peer)

    def columns(c):
        return pl.ds(pl.multiple_of(c * w, w), w)

    def own_rows(which):
        return pl.ds(pl.multiple_of((2 * z + which) * depth, depth), depth)

    def load_weight(c, which):
        source = (gate_hbm, up_hbm)[which]
        return pltpu.make_async_copy(
            source.at[:, columns(c)],
            weights.at[c, own_rows(core), pl.ds(which * w, w)],
            weight_load.at[c, which],
        )

    def load_rows(which):
        return pltpu.make_async_copy(
            (later_hbm, earlier_hbm)[which], (later_v, earlier_v)[which], rows_load.at[which]
        )

    def load_cot(c):
        return pltpu.make_async_copy(cot_hbm.at[:, columns(c)], cot_v.at[c], cot_load.at[c])

    def load_mix(which):
        sources = (taps_hbm, bias_hbm, taps_sum_hbm, bias_sum_hbm)
        targets = (taps_ref, bias_ref, taps_sum_ref, bias_sum_ref)
        return pltpu.make_async_copy(sources[which], targets[which], mix_load.at[which])

    def load_sum(which):
        return pltpu.make_async_copy(
            (gate_sum_hbm, up_sum_hbm)[which], (gate_out, up_out)[which], sum_load.at[which]
        )

    def block_of(half, i):
        return pl.ds(pl.multiple_of((half * side + i) * r, r), r)

    def piece(half, i, p):
        return block_of(half, i), pl.ds(pl.multiple_of(p * cut, cut), cut)

    def remote(source, target, send, recv, device):
        return pltpu.make_async_remote_copy(
            src_ref=source,
            dst_ref=target,
            send_sem=send,
            recv_sem=recv,
            device_id=device,
            device_id_type=MESH,
        )

    def shard(o, which, c):
        return weights.at[c, pl.ds(pl.multiple_of((2 * o + which) * depth, depth), depth)]

    def line_copy(way, o, c):
        ref = shard(o, core, c)
        return remote(
            ref, ref, line_send.at[way, c, o], line_recv.at[c, o], {"fs": neighbours[way]}
        )

    def pair_copy(o, which, c):
        ref = shard(o, which, c)
        return remote(ref, ref, pair_send.at[c, o], pair_recv.at[c, o], {"fs": partner})

    def term_copy(c):
        return remote(
            out_t.at[lax.rem(c, 2)],
            pair_t.at[c],
            term_send.at[c],
            term_recv.at[c],
            {"fs": partner},
        )

    def ring_slot(way, c, d):
        return ring.at[way, c, d - 1 if way == 0 else d]

    def ring_copy(way, c, d):
        at = (way, c, d - 1 if way == 0 else d)
        slot = ring.at[at]
        return remote(slot, slot, ring_send.at[at], ring_recv.at[at], {"fs": neighbours[way]})

    def source_of(half, i, p):
        if isinstance(p, int) and p == q:
            return help_in.at[block_of(half, i)]
        return rows_s.at[piece(half, i, p)]

    def target_of(half, i, p):
        if isinstance(p, int) and p == q:
            return help_out.at[block_of(half, i)]
        return rows_out.at[piece(half, i, p)]

    def first_copy(half, k, p):
        peer, device = first_peer(half, k)
        at = (half, k - 1, p)
        return remote(
            source_of(half, peer, p),
            first_in.at[at],
            first_send.at[at],
            first_recv.at[at],
            {"tp": device},
        )

    def second_copy(half, k, p, position):
        _, device = second_peer(half, k)
        slot = second_in.at[half, position, p]
        at = (half, k - 1, p)
        return remote(slot, slot, second_send.at[at], second_recv.at[at], {"tp": device})

    def third_copy(half, k, p, shown):
        _, device = first_peer(half, k)
        ref = target_of(half, shown, p)
        at = (half, k - 1, p)
        return remote(ref, ref, third_send.at[at], third_recv.at[at], {"tp": device})

    def help_copy():
        device = jnp.where(z == 0, neighbours[0], neighbours[1])
        source = rows_s.at[:, pl.ds(0, cut)]
        return remote(source, help_in, help_send.at[0], help_recv.at[0], {"fs": device})

    def back_copy(half, i):
        device = jnp.where(z == 1, neighbours[1], neighbours[0])
        at = (half, i)
        return remote(
            help_out.at[block_of(half, i)],
            rows_out.at[piece(half, i, 0)],
            back_send.at[at],
            back_recv.at[at],
            {"fs": device},
        )

    def small_pair():
        return remote(small_v, small_in, small_send.at[2, 0], small_recv.at[z], {"fs": partner})

    def small_copy(way, o):
        ref = small_buf.at[o]
        return remote(
            ref, ref, small_send.at[way, o], small_recv.at[o], {"fs": neighbours[way]}
        )

    def send_small():
        small_pair().wait_recv()
        low = jnp.where(core == 0, small_v[...], small_in[...])
        high = jnp.where(core == 0, small_in[...], small_v[...])
        small_buf[z] = low + high

        @pl.when(z < last)
        def _():
            small_copy(0, z).start()

        @pl.when(z > 0)
        def _():
            small_copy(1, z).start()

    def pass_small(k):
        @pl.when(z - k >= 0)
        def _():
            small_copy(0, z - k).wait_recv()

            @pl.when(z < last)
            def _():
                small_copy(0, z - k).start()

        @pl.when(z + k <= last)
        def _():
            small_copy(1, z + k).wait_recv()

            @pl.when(z > 0)
            def _():
                small_copy(1, z + k).start()

    for c in range(n):
        load_weight(c, 0).start()
        load_weight(c, 1).start()

    barrier = pltpu.get_barrier_semaphore()
    def greet(device):
        pl.semaphore_signal(barrier, inc=1, device_id={"fs": device}, device_id_type=MESH)

    @pl.when(z < last)
    def _():
        greet(neighbours[0])

    @pl.when(z > 0)
    def _():
        greet(neighbours[1])

    greet(partner)
    for half in range(2):
        for k in range(1, side):
            pl.semaphore_signal(
                barrier, inc=1, device_id={"tp": first_peer(half, k)[1]}, device_id_type=MESH
            )

    load_rows(1).start()
    for c in range(n):
        load_cot(c).start()
    load_rows(0).start()
    for which in range(4):
        load_mix(which).start()
    load_sum(0).start()
    load_sum(1).start()

    expected = 1 + 2 * (side - 1) + jnp.where(z < last, 1, 0) + jnp.where(z > 0, 1, 0)
    pl.semaphore_wait(barrier, expected)

    block = math.gcd(tokens, FORWARD_ROWS)

    def forward(rows_v, c):
        def body(index, carry):
            rows = pl.ds(pl.multiple_of(index * block, block), block)
            value = jnp.dot(rows_v[rows, :], weights[c], preferred_element_type=F32)
            pre[rows, :] = value.astype(BF16)
            return carry

        lax.fori_loop(0, tokens // block, body, 0)

    def mixing(c):
        gate = pre[:, :w].astype(F32)
        value = pre[:, w:].astype(F32)
        taps = [taps_ref[k : k + 1, columns(c)] for k in range(count)]
        shifted = [down(gate, count - 1 - k) for k in range(count)]
        mixed = bias_ref[:, columns(c)] + taps[0] * shifted[0]
        for k in range(1, count):
            mixed += taps[k] * shifted[k]
        sig = jax.nn.sigmoid(mixed)
        return value, taps, shifted, mixed, sig

    def middle_later(c):
        value, _, _, mixed, sig = mixing(c)
        hidden_out[:, columns(c)] = (mixed * sig * value).astype(BF16)

    def middle_earlier(c):
        value, taps, shifted, mixed, sig = mixing(c)
        cot = cot_v[c].astype(F32)
        grads[c, :, w:] = (cot * (mixed * sig)).astype(BF16)
        mixed_grad = cot * value * sig * (1.0 + mixed * (1.0 - sig))
        total = taps[count - 1] * mixed_grad
        for k in range(count - 1):
            total += taps[k] * up(mixed_grad, count - 1 - k)
        grads[c, :, :w] = total.astype(BF16)
        for k in range(count):
            small_v[c, k : k + 1, :] = jnp.sum(mixed_grad * shifted[k], axis=0, keepdims=True)
        small_v[c, count : count + 1, :] = jnp.sum(mixed_grad, axis=0, keepdims=True)

    def rows_part(c, chunks, cols):
        value = contract_last(grads[c - chunks + 1], weights[c - chunks + 1, cols, :])
        for k in range(1, chunks):
            at = c - chunks + 1 + k
            value += contract_last(grads[at], weights[at, cols, :])
        return value

    def add_rows(c):
        wide = math.gcd(model, 512)

        def body(p, carry):
            cols = pl.ds(pl.multiple_of(p * wide, wide), wide)
            acc[:, cols] += rows_part(c, group, cols)
            return carry

        lax.fori_loop(0, model // wide, body, 0)

    def kept(p):
        return jnp.logical_not(jnp.logical_and(helped, jnp.logical_and(at_end, p == 0)))

    def start_first(p):
        @pl.when(kept(p))
        def _():
            for k in range(1, side):
                for half in range(2):
                    first_copy(half, k, p).start()

        @pl.when(jnp.logical_not(kept(p)))
        def _():
            help_copy().start()

    def last_rows(c):
        def body(p, carry):
            cols = pl.ds(pl.multiple_of(p * cut, cut), cut)
            rows_s[:, cols] = (acc[:, cols] + rows_part(c, tail, cols)).astype(BF16)
            start_first(p)
            return carry

        lax.fori_loop(0, q, body, 0)

    def make_terms(c, carry):
        slot = lax.rem(c, 2)

        @pl.when(c >= 2)
        def _():
            term_copy(c - 2).wait_send()

        half_rows = chips * depth
        value = jnp.dot(earlier_t[...], grads[c], preferred_element_type=F32)
        out_t[slot] = value[:half_rows].astype(BF16)
        own_t[c] = value[half_rows:].astype(BF16)
        term_copy(c).start()
        return carry

    def wait_terms(c, carry):
        term_copy(c).wait_recv()
        return carry

    def transpose_rows():
        acc[...] = jnp.zeros_like(acc)
        small_v[...] = jnp.zeros_like(small_v)

        def body(d, carry):
            cols = pl.ds(pl.multiple_of(d * 2 * depth, 2 * depth), 2 * depth)
            value = earlier_v[:, cols].T
            for which in range(2):
                owner = jnp.where(core == which, chips + d, d)
                rows = pl.ds(pl.multiple_of(owner * depth, depth), depth)
                earlier_t[rows, :] = value[which * depth : (which + 1) * depth]
            return carry

        lax.fori_loop(0, chips, body, 0)

    def compute_first(c):
        @pl.when(c == 0)
        def _():
            load_rows(1).wait()
            for which in range(4):
                load_mix(which).wait()
            load_sum(0).wait()
            load_sum(1).wait()
            transpose_rows()

        for o in range(chips):
            pair_copy(o, 1 - core, c).wait_recv()
        forward(earlier_v, c)

    def compute_second(c):
        load_cot(c).wait()
        middle_earlier(c)

        @pl.when(jnp.logical_and(c < n - tail, lax.rem(c, group) == group - 1))
        def _():
            add_rows(c)

        @pl.when(c == n - 1)
        def _():
            last_rows(c)
            small_pair().start()

    def compute_later(c):
        @pl.when(c == 0)
        def _():
            load_rows(0).wait()

        forward(later_v, c)
        middle_later(c)

    def arrive(way, o, c, goes_on):
        line_copy(way, o, c).wait_recv()

        @pl.when(goes_on)
        def _():
            line_copy(way, o, c).start()

        pair_copy(o, core, c).start()

    def terms_of(c, d):
        rows = pl.ds(pl.multiple_of(d * depth, depth), depth)
        return own_t[c, rows, :].astype(F32) + pair_t[c, rows, :].astype(F32)

    def push(way, c, d, first_on_line):
        slot = ring_slot(way, c, d)

        @pl.when(first_on_line)
        def _():
            slot[...] = terms_of(c, d).astype(BF16)

        @pl.when(jnp.logical_not(first_on_line))
        def _():
            ring_copy(way, c, d).wait_recv()
            slot[...] = (terms_of(c, d) + slot[...].astype(F32)).astype(BF16)

        ring_copy(way, c, d).start()

    def push_up(c, carry):
        for d in range(last, 0, -1):

            @pl.when(d > z)
            def _():
                push(0, c, d, z == 0)

        return carry

    def push_down(c, carry):
        for d in range(last):

            @pl.when(d < z)
            def _():
                push(1, c, d, z == last)

        return carry

    def finish_sum(c, carry):
        def add(value):
            gate_out[:, columns(c)] += sizes.scale * value[:, :w]
            up_out[:, columns(c)] += sizes.scale * value[:, w:]

        base = terms_of(c, z)

        @pl.when(z == 0)
        def _():
            ring_copy(1, c, z).wait_recv()
            add(base + ring_slot(1, c, z)[...].astype(F32))

        @pl.when(z == last)
        def _():
            ring_copy(0, c, z).wait_recv()
            add(base + ring_slot(0, c, z)[...].astype(F32))

        @pl.when(jnp.logical_and(z > 0, z < last))
        def _():
            ring_copy(0, c, z).wait_recv()
            ring_copy(1, c, z).wait_recv()
            add(
                base
                + ring_slot(0, c, z)[...].astype(F32)
                + ring_slot(1, c, z)[...].astype(F32)
            )

        return carry

    far = jnp.maximum(z, last - z)

    def termed(i):
        return jnp.where(i >= n, n, jnp.clip(i, 0, max(n - 2, 0)))

    def pushed(i, hops):
        turn = i - (n - 1)
        near = jnp.clip(jnp.maximum(3 + (turn - 1) // 2, turn - 2), 0, n)
        near = jnp.where(turn >= 1, near, 0)
        after = jnp.where(hops == 1, near, jnp.clip(turn + 1 - 2 * hops, 0, n))
        return jnp.where(hops == 0, termed(i), after)

    batch = math.gcd(q, 2)
    rounds = q // batch

    hold = jnp.where(helper, rounds - 1, 0)
    turns = max(n + 4, n + 2 * (last - 1), 6 + 2 * last, 3 * rounds, 2 * rounds + 3)
    end = n - 1 + turns

    def exchange(j):
        def during(first, action):
            @pl.when(jnp.logical_and(j > first, j <= first + rounds))
            def _():
                for at in range(batch):
                    p = (j - 1 - first) * batch + at

                    @pl.when(kept(p))
                    def _():
                        for half in range(2):
                            action(half, p)

        during(0, exchange_first)
        during(rounds, exchange_second)
        if helped:
            assist(j - 2 * rounds)
        during(rounds + hold, exchange_send)

    def assist(turn):
        @pl.when(jnp.logical_and(helper, turn == 0))
        def _():
            help_copy().wait_recv()
            for k in range(1, side):
                for half in range(2):
                    first_copy(half, k, q).start()

        @pl.when(jnp.logical_and(helper, turn == 1))
        def _():
            for half in range(2):
                exchange_first(half, q)

        @pl.when(jnp.logical_and(helper, turn == 2))
        def _():
            for half in range(2):
                exchange_second(half, q)
                exchange_send(half, q)
                back_copy(half, firsts[half]).start()

        @pl.when(jnp.logical_and(helper, turn == 3))
        def _():
            for half in range(2):
                for k in range(1, side):
                    shown = lax.rem(firsts[half] + side - k, side)
                    third_copy(half, k, q, shown).wait_recv()
                    back_copy(half, shown).start()

    def exchange_first(half, p):
        total = source_of(half, firsts[half], p)[...].astype(F32)
        for k in range(1, side):
            first_copy(half, k, p).wait_recv()
            total += first_in[half, k - 1, p].astype(F32)
        second_in[half, seconds[half], p] = total.astype(BF16)
        for k in range(1, side):
            second_copy(half, k, p, seconds[half]).start()

    def exchange_second(half, p):
        for k in range(1, side):
            position = lax.rem(seconds[half] + side - k, side)
            second_copy(half, k, p, position).wait_recv()
        total = second_in[half, 0, p].astype(F32)
        for position in range(1, side):
            total += second_in[half, position, p].astype(F32)
        target_of(half, firsts[half], p)[...] = total.astype(BF16)

    def exchange_send(half, p):
        for k in range(1, side):
            third_copy(half, k, p, firsts[half]).start()

    def exchange_third(half, p):
        for k in range(1, side):
            third_copy(half, k, p, lax.rem(firsts[half] + side - k, side)).wait_recv()

    def finish_small():
        for c in range(n):
            total = small_buf[0, c]
            for source in range(1, chips):
                total += small_buf[source, c]
            total = sizes.scale * total
            cols = slice(c * w, (c + 1) * w)
            taps_out[:, cols] = taps_sum_ref[:, cols] + total[:count]
            bias_out[:, cols] = bias_sum_ref[:, cols] + total[count : count + 1]
        small_pair().wait_send()

    def drain_gather(c, carry):
        def over_chips(d, inner):
            pair_copy(d, core, c).wait_send()

            @pl.when(jnp.logical_and(d <= z, z < last))
            def _():
                line_copy(0, d, c).wait_send()

            @pl.when(jnp.logical_and(d >= z, z > 0))
            def _():
                line_copy(1, d, c).wait_send()

            return inner

        return lax.fori_loop(0, chips, over_chips, carry)

    def drain_ring(c, carry):
        for d in range(chips):
            if d > 0:

                @pl.when(d > z)
                def _():
                    ring_copy(0, c, d).wait_send()

            if d < last:

                @pl.when(d < z)
                def _():
                    ring_copy(1, c, d).wait_send()

        return carry

    def drain_first():
        for p in range(q):

            @pl.when(kept(p))
            def _():
                for half in range(2):
                    for k in range(1, side):
                        first_copy(half, k, p).wait_send()

    def drain_second():
        for p in range(q):

            @pl.when(kept(p))
            def _():
                for half in range(2):
                    for k in range(1, side):
                        second_copy(half, k, p, seconds[half]).wait_send()

    def drain_early(j):
        @pl.when(j == rounds)
        def _():
            lax.fori_loop(0, n, drain_gather, 0)
            for c in range(max(n - 2, 0), n):
                term_copy(c).wait_send()

        @pl.when(j == 2 * rounds + 1)
        def _():
            drain_first()

    def drain_late():
        lax.fori_loop(0, n - 1, drain_ring, 0)
        drain_second()
        finish_small()

    def send_own(c, carry):
        load_weight(c, 0).wait()
        load_weight(c, 1).wait()

        @pl.when(z < last)
        def _():
            line_copy(0, z, c).start()

        @pl.when(z > 0)
        def _():
            line_copy(1, z, c).start()

        pair_copy(z, core, c).start()
        return carry

    @pl.when(at_end)
    def _():
        lax.fori_loop(0, n, send_own, 0)

    def step(s, carry):
        i = s - far

        @pl.when(jnp.logical_and(s < n, jnp.logical_not(at_end)))
        def _():
            send_own(s, 0)

        for k in range(1, chips):
            c = s - k
            inside = jnp.logical_and(c >= 0, c < n)

            @pl.when(jnp.logical_and(inside, z - k >= 0))
            def _():
                arrive(0, z - k, c, z < last)

            @pl.when(jnp.logical_and(inside, z + k <= last))
            def _():
                arrive(1, z + k, c, z > 0)

        lax.fori_loop(termed(i - 1), termed(i), make_terms, 0)

        @pl.when(jnp.logical_and(i >= 0, i < n))
        def _():
            compute_first(i)

        drain_early(i - (n - 1))
        exchange(i - (n - 1))
        lax.fori_loop(termed(i - 1), termed(i), wait_terms, 0)
        @pl.when(i == n)
        def _():
            send_small()

        turn = i - (n + 4)
        inside = jnp.logical_and(turn >= 2, turn <= 2 * last)

        @pl.when(jnp.logical_and(inside, lax.rem(turn, 2) == 0))
        def _():
            pass_small(turn // 2)

        lax.fori_loop(pushed(i - 1, z), pushed(i, z), push_up, 0)
        lax.fori_loop(pushed(i - 1, last - z), pushed(i, last - z), push_down, 0)
        finish = jnp.where(at_end, i - 1, i)
        hops = jnp.where(at_end, 2, far)
        lax.fori_loop(pushed(finish - 1, hops), pushed(finish, hops), finish_sum, 0)

        @pl.when(i == end)
        def _():
            drain_late()

        @pl.when(jnp.logical_and(i >= 0, i < n))
        def _():
            compute_second(i)

        @pl.when(jnp.logical_and(i >= n, i < 2 * n))
        def _():
            compute_later(i - n)

        return carry

    lax.fori_loop(0, end + last + 1, step, 0)

    lax.fori_loop(n - 1, n, drain_ring, 0)

    def drain_small(o, carry):
        @pl.when(jnp.logical_and(o <= z, z < last))
        def _():
            small_copy(0, o).wait_send()

        @pl.when(jnp.logical_and(o >= z, z > 0))
        def _():
            small_copy(1, o).wait_send()

        return carry

    lax.fori_loop(0, chips, drain_small, 0)
    for p in range(q):

        @pl.when(kept(p))
        def _():
            for half in range(2):
                exchange_third(half, p)
                for k in range(1, side):
                    third_copy(half, k, p, firsts[half]).wait_send()

    if helped:

        @pl.when(at_end)
        def _():
            help_copy().wait_send()
            for half in range(2):
                for i in range(side):
                    back_copy(half, i).wait_recv()

        @pl.when(helper)
        def _():
            for half in range(2):
                for k in range(1, side):
                    first_copy(half, k, q).wait_send()
                    second_copy(half, k, q, seconds[half]).wait_send()
                    third_copy(half, k, q, firsts[half]).wait_send()
                for i in range(side):
                    back_copy(half, i).wait_send()


def store_kernel(*refs):
    count = len(refs) // 2
    sources, targets, sems = refs[:count], refs[count : 2 * count], refs[-1]
    copies = [
        pltpu.make_async_copy(sources[at], targets[at], sems.at[at]) for at in range(count)
    ]
    for copy in copies:
        copy.start()
    for copy in copies:
        copy.wait()


def on_device(
    rows_later,
    rows_earlier,
    out_cotangent,
    gate_proj,
    up_proj,
    conv_taps,
    conv_bias,
    gate_grad_sum,
    up_grad_sum,
    taps_grad_sum,
    bias_grad_sum,
):
    tokens, model = rows_later.shape
    depth, width = gate_proj.shape
    taps = conv_taps.shape[0]
    sizes = Sizes(
        lax.axis_size("fs"), lax.axis_size("tp"), tokens, model, depth, width, taps
    )
    n, w, q, r, cut = sizes.n, sizes.w, sizes.q, sizes.r, sizes.cut
    chips, side, fs_size = sizes.chips, sizes.side, sizes.fs_size
    dma = pltpu.SemaphoreType.DMA
    whole = pl.BlockSpec(memory_space=pltpu.VMEM)
    far = pl.BlockSpec(memory_space=pl.ANY)
    links = max(side - 1, 1)
    outs = pl.pallas_call(
        functools.partial(kernel, sizes),
        out_shape=(
            pltpu.VMEM((tokens, width), BF16),
            pltpu.VMEM((tokens, model), BF16),
            pltpu.VMEM((depth, width), F32),
            pltpu.VMEM((depth, width), F32),
            pltpu.VMEM((taps, width), F32),
            pltpu.VMEM((1, width), F32),
        ),
        in_specs=[far] * 11,
        out_specs=(whole,) * 6,
        scratch_shapes=[
            pltpu.VMEM((tokens, model), BF16),
            pltpu.VMEM((tokens, model), BF16),
            pltpu.VMEM((model, tokens), BF16),
            pltpu.VMEM((n, tokens, w), BF16),
            pltpu.VMEM((n, model, 2 * w), BF16),
            pltpu.VMEM((tokens, 2 * w), BF16),
            pltpu.VMEM((n, tokens, 2 * w), BF16),
            pltpu.VMEM((tokens, model), F32),
            pltpu.VMEM((n, chips * depth, 2 * w), BF16),
            pltpu.VMEM((2, chips * depth, 2 * w), BF16),
            pltpu.VMEM((n, chips * depth, 2 * w), BF16),
            pltpu.VMEM((2, n, max(chips - 1, 1), depth, 2 * w), BF16),
            pltpu.VMEM((tokens, model), BF16),
            pltpu.VMEM((tokens, cut), BF16),
            pltpu.VMEM((tokens, cut), BF16),
            dma((1,)),
            dma((1,)),
            dma((2, side)),
            dma((2, side)),
            pltpu.VMEM((2, links, q + 1, r, cut), BF16),
            pltpu.VMEM((2, side, q + 1, r, cut), BF16),
            pltpu.VMEM((n, 8 * -(-(taps + 1) // 8), w), F32),
            pltpu.VMEM((n, 8 * -(-(taps + 1) // 8), w), F32),
            pltpu.VMEM((chips, n, 8 * -(-(taps + 1) // 8), w), F32),
            pltpu.VMEM((taps, width), F32),
            pltpu.VMEM((1, width), F32),
            pltpu.VMEM((taps, width), F32),
            pltpu.VMEM((1, width), F32),
            dma((4,)),
            dma((n, 2)),
            dma((2,)),
            dma((n,)),
            dma((2,)),
            dma((2, n, chips)),
            dma((n, chips)),
            dma((n, chips)),
            dma((n, chips)),
            dma((n,)),
            dma((n,)),
            dma((2, n, max(chips - 1, 1))),
            dma((2, n, max(chips - 1, 1))),
        ]
        + [dma((2, links, q + 1))] * 6
        + [dma((3, chips)), dma((chips,))],
        compiler_params=pltpu.CompilerParams(
            collective_id=0, has_side_effects=True, vmem_limit_bytes=VMEM_BYTES
        ),
    )(
        rows_later,
        rows_earlier,
        out_cotangent,
        gate_proj,
        up_proj,
        gate_grad_sum,
        up_grad_sum,
        conv_taps,
        conv_bias[None],
        taps_grad_sum,
        bias_grad_sum[None],
    )
    stored = pl.pallas_call(
        store_kernel,
        out_shape=tuple(jax.ShapeDtypeStruct(out.shape, out.dtype) for out in outs),
        in_specs=[whole] * len(outs),
        out_specs=(far,) * len(outs),
        scratch_shapes=[dma((len(outs),))],
        compiler_params=pltpu.CompilerParams(vmem_limit_bytes=1024 * 1024),
    )(*[pltpu.with_memory_space_constraint(out, pltpu.VMEM) for out in outs])
    return stored[:5] + (stored[5][0],)


def solution(mesh):
    placed = (
        P("fs", None),
        P("fs", None),
        P("fs", "tp"),
        P("fs", "tp"),
        P("fs", "tp"),
        P(None, "tp"),
        P("tp"),
        P("fs", "tp"),
        P("fs", "tp"),
        P(None, "tp"),
        P("tp"),
    )
    return jax.shard_map(
        on_device,
        mesh=mesh,
        in_specs=placed,
        out_specs=(
            P("fs", "tp"),
            P("fs", None),
            P("fs", "tp"),
            P("fs", "tp"),
            P(None, "tp"),
            P("tp"),
        ),
        check_vma=False,
    )
```

```python
import functools
import math

import jax
import jax.numpy as jnp
from jax import lax
from jax.experimental import pallas as pl
from jax.experimental.pallas import tpu as pltpu
from jax.sharding import PartitionSpec as P

MESH = pl.DeviceIdType.MESH
VMEM_BYTES = 57 * 1024 * 1024
FORWARD_ROWS = 768
F32, BF16 = jnp.float32, jnp.bfloat16


def contract_last(left, right):
    return lax.dot_general(
        left, right, (((1,), (1,)), ((), ())), preferred_element_type=jnp.float32
    )


def down(values, distance):
    if distance == 0:
        return values
    index = lax.broadcasted_iota(jnp.int32, values.shape, 0)
    return jnp.where(index >= distance, pltpu.roll(values, distance, 0), 0.0)


def up(values, distance):
    if distance == 0:
        return values
    rows = values.shape[0]
    index = lax.broadcasted_iota(jnp.int32, values.shape, 0)
    return jnp.where(index < rows - distance, pltpu.roll(values, rows - distance, 0), 0.0)


class Sizes:
    def __init__(self, fs_size, tp_size, tokens, model, depth, width, taps):
        self.fs_size = fs_size
        self.chips = fs_size // 2
        self.side = math.isqrt(tp_size)
        self.tokens, self.model, self.depth, self.width = tokens, model, depth, width
        self.w = math.gcd(width, 128)
        self.n = width // self.w
        self.taps = taps
        self.group = math.gcd(self.n, 2)
        self.tail = min(self.n, 2 * self.group)
        self.r = tokens // (2 * self.side)
        self.q = max(q for q in (1, 2, 4, 8) if model % (128 * q) == 0)
        self.cut = model // self.q
        self.scale = 1.0 / math.sqrt(tokens * fs_size)


def kernel(
    sizes,
    later_hbm,
    earlier_hbm,
    cot_hbm,
    gate_hbm,
    up_hbm,
    gate_sum_hbm,
    up_sum_hbm,
    taps_hbm,
    bias_hbm,
    taps_sum_hbm,
    bias_sum_hbm,
    hidden_out,
    rows_out,
    gate_out,
    up_out,
    taps_out,
    bias_out,
    later_v,
    earlier_v,
    earlier_t,
    cot_v,
    weights,
    pre,
    grads,
    acc,
    own_t,
    out_t,
    pair_t,
    ring,
    rows_s,
    help_in,
    help_out,
    help_send,
    help_recv,
    back_send,
    back_recv,
    first_in,
    second_in,
    small_v,
    small_in,
    small_buf,
    taps_ref,
    bias_ref,
    taps_sum_ref,
    bias_sum_ref,
    mix_load,
    weight_load,
    rows_load,
    cot_load,
    sum_load,
    line_send,
    line_recv,
    pair_send,
    pair_recv,
    term_send,
    term_recv,
    ring_send,
    first_send,
    first_recv,
    second_send,
    second_recv,
    third_send,
    third_recv,
    small_send,
    small_recv,
):
    n, w, q, r, cut = sizes.n, sizes.w, sizes.q, sizes.r, sizes.cut
    group, tail = sizes.group, sizes.tail
    chips, side, depth = sizes.chips, sizes.side, sizes.depth
    fs_size, tokens, model = sizes.fs_size, sizes.tokens, sizes.model
    count = sizes.taps
    last = chips - 1
    fs = lax.axis_index("fs")
    tp = lax.axis_index("tp")
    z = fs // 2
    core = lax.rem(fs, 2)
    partner = 2 * z + 1 - core
    at_end = jnp.logical_or(z == 0, z == last)
    helped = chips >= 4
    helper = jnp.logical_and(helped, jnp.logical_or(z == 1, z == last - 1))
    neighbours = (lax.rem(fs + 2, fs_size), lax.rem(fs + fs_size - 2, fs_size))
    ty = tp // side
    tx = lax.rem(tp, side)
    firsts = (tx, ty)
    seconds = (ty, tx)

    def first_peer(half, k):
        peer = lax.rem(firsts[half] + k, side)
        return peer, (ty * side + peer if half == 0 else peer * side + tx)

    def second_peer(half, k):
        peer = lax.rem(seconds[half] + k, side)
        return peer, (peer * side + tx if half == 0 else ty * side + peer)

    def columns(c):
        return pl.ds(pl.multiple_of(c * w, w), w)

    def own_rows(which):
        return pl.ds(pl.multiple_of((2 * z + which) * depth, depth), depth)

    def load_weight(c, which):
        source = (gate_hbm, up_hbm)[which]
        return pltpu.make_async_copy(
            source.at[:, columns(c)],
            weights.at[c, own_rows(core), pl.ds(which * w, w)],
            weight_load.at[which],
        )

    def wait_weights():
        for which in range(2):
            ref = weights.at[:, own_rows(core), pl.ds(which * w, w)]
            pltpu.make_async_copy(ref, ref, weight_load.at[which]).wait()

    def load_rows(which):
        return pltpu.make_async_copy(
            (later_hbm, earlier_hbm)[which], (later_v, earlier_v)[which], rows_load.at[which]
        )

    def load_cot():
        return pltpu.make_async_copy(cot_hbm, cot_v, cot_load.at[0])

    def load_mix(which):
        sources = (taps_hbm, bias_hbm, taps_sum_hbm, bias_sum_hbm)
        targets = (taps_ref, bias_ref, taps_sum_ref, bias_sum_ref)
        return pltpu.make_async_copy(sources[which], targets[which], mix_load.at[which])

    def load_sum(which):
        return pltpu.make_async_copy(
            (gate_sum_hbm, up_sum_hbm)[which], (gate_out, up_out)[which], sum_load.at[which]
        )

    def block_of(half, i):
        return pl.ds(pl.multiple_of((half * side + i) * r, r), r)

    def piece(half, i, p):
        return block_of(half, i), pl.ds(pl.multiple_of(p * cut, cut), cut)

    def remote(source, target, send, recv, device):
        return pltpu.make_async_remote_copy(
            src_ref=source,
            dst_ref=target,
            send_sem=send,
            recv_sem=recv,
            device_id=device,
            device_id_type=MESH,
        )

    def shard(o, which, c):
        return weights.at[c, pl.ds(pl.multiple_of((2 * o + which) * depth, depth), depth)]

    def line_copy(way, o, c):
        ref = shard(o, core, c)
        return remote(
            ref, ref, line_send.at[way, o], line_recv.at[c, o], {"fs": neighbours[way]}
        )

    def line_sent(way, o):
        rows = pl.ds(pl.multiple_of((2 * o + core) * depth, depth), depth)
        ref = weights.at[:, rows]
        return remote(
            ref, ref, line_send.at[way, o], line_recv.at[0, 0], {"fs": neighbours[way]}
        )

    def pair_copy(o, c):
        ref = shard(o, core, c)
        return remote(ref, ref, pair_send.at[0], pair_recv.at[c], {"fs": partner})

    def pair_received(c):
        ref = weights.at[c, pl.ds(0, chips * depth)]
        return remote(ref, ref, pair_send.at[0], pair_recv.at[c], {"fs": partner})

    def pair_sent():
        ref = weights.at[:, pl.ds(0, chips * depth)]
        return remote(ref, ref, pair_send.at[0], pair_recv.at[0], {"fs": partner})

    def term_copy(c):
        return remote(
            out_t.at[lax.rem(c, 2)],
            pair_t.at[c],
            term_send.at[lax.rem(c, 2)],
            term_recv.at[c],
            {"fs": partner},
        )

    def ring_slot(way, c, d):
        return ring.at[way, c, d - 1 if way == 0 else d]

    def ring_copy(way, c, d, at):
        index = d - 1 if way == 0 else d
        recv = line_recv.at[c, jnp.where(d == at, chips + way, d)]
        slot = ring.at[way, c, index]
        return remote(
            slot,
            slot,
            ring_send.at[way, index],
            recv,
            {"fs": neighbours[way]},
        )

    def ring_sent(way, d):
        index = d - 1 if way == 0 else d
        ref = ring.at[way, :, index]
        return remote(
            ref, ref, ring_send.at[way, index], line_recv.at[0, 0], {"fs": neighbours[way]}
        )

    def extra(p):
        return int(isinstance(p, int) and p == q)

    def source_of(half, i, p):
        if isinstance(p, int) and p == q:
            return help_in.at[block_of(half, i)]
        return rows_s.at[piece(half, i, p)]

    def target_of(half, i, p):
        if isinstance(p, int) and p == q:
            return help_out.at[block_of(half, i)]
        return rows_out.at[piece(half, i, p)]

    def first_copy(half, k, p):
        peer, device = first_peer(half, k)
        at = (half, k - 1, p)
        return remote(
            source_of(half, peer, p),
            first_in.at[at],
            first_send.at[half, k - 1, extra(p)],
            first_recv.at[at],
            {"tp": device},
        )

    def second_copy(half, k, p, position):
        _, device = second_peer(half, k)
        slot = second_in.at[half, position, p]
        at = (half, k - 1, p)
        return remote(
            slot, slot, second_send.at[half, k - 1, extra(p)], second_recv.at[at], {"tp": device}
        )

    def third_copy(half, k, p, shown):
        _, device = first_peer(half, k)
        ref = target_of(half, shown, p)
        at = (half, k - 1, extra(p))
        return remote(ref, ref, third_send.at[at], third_recv.at[at], {"tp": device})

    def first_sent(half, k, skip):
        peer, device = first_peer(half, k)
        ref = rows_s.at[block_of(half, peer), pl.ds(skip * cut, model - skip * cut)]
        at = (half, k - 1, 0)
        return remote(ref, ref, first_send.at[at], first_recv.at[at], {"tp": device})

    def second_sent(half, k, skip):
        _, device = second_peer(half, k)
        ref = second_in.at[half, seconds[half], pl.ds(skip, q - skip)]
        at = (half, k - 1, 0)
        return remote(ref, ref, second_send.at[at], second_recv.at[at], {"tp": device})

    def third_done(half, k, shown, skip):
        _, device = first_peer(half, k)
        ref = rows_out.at[block_of(half, shown), pl.ds(skip * cut, model - skip * cut)]
        at = (half, k - 1, 0)
        return remote(ref, ref, third_send.at[at], third_recv.at[at], {"tp": device})

    def help_copy():
        device = jnp.where(z == 0, neighbours[0], neighbours[1])
        source = rows_s.at[:, pl.ds(0, cut)]
        return remote(source, help_in, help_send.at[0], help_recv.at[0], {"fs": device})

    def back_copy(half, i):
        device = jnp.where(z == 1, neighbours[1], neighbours[0])
        return remote(
            help_out.at[block_of(half, i)],
            rows_out.at[piece(half, i, 0)],
            back_send.at[0],
            back_recv.at[0],
            {"fs": device},
        )

    def back_done():
        device = jnp.where(z == 1, neighbours[1], neighbours[0])
        target = rows_out.at[:, pl.ds(0, cut)]
        return remote(help_out, target, back_send.at[0], back_recv.at[0], {"fs": device})

    def small_pair():
        return remote(small_v, small_in, small_send.at[2, 0], small_recv.at[z], {"fs": partner})

    def small_copy(way, o):
        ref = small_buf.at[o]
        return remote(
            ref, ref, small_send.at[way, o], small_recv.at[o], {"fs": neighbours[way]}
        )

    def send_small():
        small_pair().wait_recv()
        low = jnp.where(core == 0, small_v[...], small_in[...])
        high = jnp.where(core == 0, small_in[...], small_v[...])
        small_buf[z] = low + high

        @pl.when(z < last)
        def _():
            small_copy(0, z).start()

        @pl.when(z > 0)
        def _():
            small_copy(1, z).start()

    def pass_small(k):
        @pl.when(z - k >= 0)
        def _():
            small_copy(0, z - k).wait_recv()

            @pl.when(z < last)
            def _():
                small_copy(0, z - k).start()

        @pl.when(z + k <= last)
        def _():
            small_copy(1, z + k).wait_recv()

            @pl.when(z > 0)
            def _():
                small_copy(1, z + k).start()

    for c in range(n):
        load_weight(c, 0).start()
        load_weight(c, 1).start()

    barrier = pltpu.get_barrier_semaphore()
    def greet(device):
        pl.semaphore_signal(barrier, inc=1, device_id={"fs": device}, device_id_type=MESH)

    @pl.when(z < last)
    def _():
        greet(neighbours[0])

    @pl.when(z > 0)
    def _():
        greet(neighbours[1])

    greet(partner)
    for half in range(2):
        for k in range(1, side):
            pl.semaphore_signal(
                barrier, inc=1, device_id={"tp": first_peer(half, k)[1]}, device_id_type=MESH
            )

    load_rows(1).start()
    load_cot().start()
    load_rows(0).start()
    for which in range(4):
        load_mix(which).start()
    load_sum(0).start()
    load_sum(1).start()

    expected = 1 + 2 * (side - 1) + jnp.where(z < last, 1, 0) + jnp.where(z > 0, 1, 0)
    pl.semaphore_wait(barrier, expected)
    wait_weights()

    block = math.gcd(tokens, FORWARD_ROWS)

    def forward(rows_v, c):
        def body(index, carry):
            rows = pl.ds(pl.multiple_of(index * block, block), block)
            value = jnp.dot(rows_v[rows, :], weights[c], preferred_element_type=F32)
            pre[rows, :] = value.astype(BF16)
            return carry

        lax.fori_loop(0, tokens // block, body, 0)

    def mixing(c):
        gate = pre[:, :w].astype(F32)
        value = pre[:, w:].astype(F32)
        taps = [taps_ref[k : k + 1, columns(c)] for k in range(count)]
        shifted = [down(gate, count - 1 - k) for k in range(count)]
        mixed = bias_ref[:, columns(c)] + taps[0] * shifted[0]
        for k in range(1, count):
            mixed += taps[k] * shifted[k]
        sig = jax.nn.sigmoid(mixed)
        return value, taps, shifted, mixed, sig

    def middle_later(c):
        value, _, _, mixed, sig = mixing(c)
        hidden_out[:, columns(c)] = (mixed * sig * value).astype(BF16)

    def middle_earlier(c):
        value, taps, shifted, mixed, sig = mixing(c)
        cot = cot_v[:, columns(c)].astype(F32)
        grads[c, :, w:] = (cot * (mixed * sig)).astype(BF16)
        mixed_grad = cot * value * sig * (1.0 + mixed * (1.0 - sig))
        total = taps[count - 1] * mixed_grad
        for k in range(count - 1):
            total += taps[k] * up(mixed_grad, count - 1 - k)
        grads[c, :, :w] = total.astype(BF16)
        for k in range(count):
            small_v[c, k : k + 1, :] = jnp.sum(mixed_grad * shifted[k], axis=0, keepdims=True)
        small_v[c, count : count + 1, :] = jnp.sum(mixed_grad, axis=0, keepdims=True)

    def rows_part(c, chunks, cols):
        value = contract_last(grads[c - chunks + 1], weights[c - chunks + 1, cols, :])
        for k in range(1, chunks):
            at = c - chunks + 1 + k
            value += contract_last(grads[at], weights[at, cols, :])
        return value

    def add_rows(c):
        wide = math.gcd(model, 512)

        def body(p, carry):
            cols = pl.ds(pl.multiple_of(p * wide, wide), wide)
            acc[:, cols] += rows_part(c, group, cols)
            return carry

        lax.fori_loop(0, model // wide, body, 0)

    skips = jnp.logical_and(helped, at_end)

    def kept(p):
        return jnp.logical_not(jnp.logical_and(skips, p == 0))

    def start_first(p):
        @pl.when(kept(p))
        def _():
            for k in range(1, side):
                for half in range(2):
                    first_copy(half, k, p).start()

        @pl.when(jnp.logical_not(kept(p)))
        def _():
            help_copy().start()

    def last_rows(c):
        late = q // 2

        def body(turn, carry):
            moved = jnp.where(turn < late, turn + 1, jnp.where(turn == late, 0, turn))
            p = jnp.where(skips, moved, turn)
            cols = pl.ds(pl.multiple_of(p * cut, cut), cut)
            rows_s[:, cols] = (acc[:, cols] + rows_part(c, tail, cols)).astype(BF16)
            start_first(p)
            return carry

        lax.fori_loop(0, q, body, 0)

    def make_terms(c, carry):
        slot = lax.rem(c, 2)

        @pl.when(c >= 2)
        def _():
            term_copy(c - 2).wait_send()

        half_rows = chips * depth
        value = jnp.dot(earlier_t[...], grads[c], preferred_element_type=F32)
        out_t[slot] = value[:half_rows].astype(BF16)
        own_t[c] = value[half_rows:].astype(BF16)
        term_copy(c).start()
        return carry

    def wait_terms(c, carry):
        term_copy(c).wait_recv()
        return carry

    def transpose_rows():
        acc[...] = jnp.zeros_like(acc)
        small_v[...] = jnp.zeros_like(small_v)

        def body(d, carry):
            cols = pl.ds(pl.multiple_of(d * 2 * depth, 2 * depth), 2 * depth)
            value = earlier_v[:, cols].T
            for which in range(2):
                owner = jnp.where(core == which, chips + d, d)
                rows = pl.ds(pl.multiple_of(owner * depth, depth), depth)
                earlier_t[rows, :] = value[which * depth : (which + 1) * depth]
            return carry

        lax.fori_loop(0, chips, body, 0)

    def compute_first(c):
        @pl.when(c == 0)
        def _():
            load_rows(1).wait()
            load_cot().wait()
            for which in range(4):
                load_mix(which).wait()
            load_sum(0).wait()
            load_sum(1).wait()
            transpose_rows()

        pair_received(c).wait_recv()
        forward(earlier_v, c)

    def compute_second(c):
        middle_earlier(c)

        @pl.when(jnp.logical_and(c < n - tail, lax.rem(c, group) == group - 1))
        def _():
            add_rows(c)

        @pl.when(c == n - 1)
        def _():
            last_rows(c)
            small_pair().start()

    def compute_later(c):
        @pl.when(c == 0)
        def _():
            load_rows(0).wait()

        forward(later_v, c)
        middle_later(c)

    def arrive(way, o, c, goes_on):
        line_copy(way, o, c).wait_recv()

        @pl.when(goes_on)
        def _():
            line_copy(way, o, c).start()

        pair_copy(o, c).start()

    def terms_of(c, d):
        rows = pl.ds(pl.multiple_of(d * depth, depth), depth)
        return own_t[c, rows, :].astype(F32) + pair_t[c, rows, :].astype(F32)

    def push(way, c, d, first_on_line):
        slot = ring_slot(way, c, d)

        @pl.when(first_on_line)
        def _():
            slot[...] = terms_of(c, d).astype(BF16)

        @pl.when(jnp.logical_not(first_on_line))
        def _():
            ring_copy(way, c, d, z).wait_recv()
            slot[...] = (terms_of(c, d) + slot[...].astype(F32)).astype(BF16)

        ring_copy(way, c, d, z + 1 if way == 0 else z - 1).start()

    def push_up(c, carry):
        for d in range(last, 0, -1):

            @pl.when(d > z)
            def _():
                push(0, c, d, z == 0)

        return carry

    def push_down(c, carry):
        for d in range(last):

            @pl.when(d < z)
            def _():
                push(1, c, d, z == last)

        return carry

    def finish_sum(c, carry):
        def add(value):
            gate_out[:, columns(c)] += sizes.scale * value[:, :w]
            up_out[:, columns(c)] += sizes.scale * value[:, w:]

        base = terms_of(c, z)

        @pl.when(z == 0)
        def _():
            ring_copy(1, c, z, z).wait_recv()
            add(base + ring_slot(1, c, z)[...].astype(F32))

        @pl.when(z == last)
        def _():
            ring_copy(0, c, z, z).wait_recv()
            add(base + ring_slot(0, c, z)[...].astype(F32))

        @pl.when(jnp.logical_and(z > 0, z < last))
        def _():
            ring_copy(0, c, z, z).wait_recv()
            ring_copy(1, c, z, z).wait_recv()
            add(
                base
                + ring_slot(0, c, z)[...].astype(F32)
                + ring_slot(1, c, z)[...].astype(F32)
            )

        return carry

    far = jnp.maximum(z, last - z)

    def termed(i):
        return jnp.where(i >= n, n, jnp.clip(i, 0, max(n - 2, 0)))

    def pushed(i, hops):
        turn = i - (n - 1)
        near = jnp.maximum(jnp.minimum(3 + (turn - 1) // 2, n - 2), turn - 3)
        near = jnp.where(turn >= 1, near, 0)
        turn -= 2 * (hops - 2)
        distant = jnp.maximum(jnp.minimum(turn - 3, n - 2), turn - 4)
        after = jnp.clip(jnp.where(hops == 1, near, distant), 0, n)
        return jnp.where(hops == 0, termed(i), after)

    batch = math.gcd(q, 2)
    rounds = q // batch

    hold = jnp.where(helper, rounds - 1, 0)
    turns = max(n + 5, n - 1 + 2 * last, 2 * rounds + last + 1, 3 * rounds, 2 * rounds + 3)
    end = n - 1 + turns

    def exchange(j):
        def during(first, action):
            @pl.when(jnp.logical_and(j > first, j <= first + rounds))
            def _():
                for at in range(batch):
                    p = (j - 1 - first) * batch + at

                    @pl.when(kept(p))
                    def _():
                        for half in range(2):
                            action(half, p)

        during(0, exchange_first)
        during(rounds, exchange_second)
        if helped:
            assist(j - 2 * rounds)
        during(rounds + hold, exchange_send)

    def assist(turn):
        @pl.when(jnp.logical_and(helper, turn == 0))
        def _():
            help_copy().wait_recv()
            for k in range(1, side):
                for half in range(2):
                    first_copy(half, k, q).start()

        @pl.when(jnp.logical_and(helper, turn == 1))
        def _():
            for half in range(2):
                exchange_first(half, q)

        @pl.when(jnp.logical_and(helper, turn == 2))
        def _():
            for half in range(2):
                exchange_second(half, q)
                exchange_send(half, q)
                back_copy(half, firsts[half]).start()

        @pl.when(jnp.logical_and(helper, turn == 3))
        def _():
            for half in range(2):
                for k in range(1, side):
                    shown = lax.rem(firsts[half] + side - k, side)
                    third_copy(half, k, q, shown).wait_recv()
                    back_copy(half, shown).start()

    def exchange_first(half, p):
        total = source_of(half, firsts[half], p)[...].astype(F32)
        for k in range(1, side):
            first_copy(half, k, p).wait_recv()
            total += first_in[half, k - 1, p].astype(F32)
        second_in[half, seconds[half], p] = total.astype(BF16)
        for k in range(1, side):
            second_copy(half, k, p, seconds[half]).start()

    def exchange_second(half, p):
        for k in range(1, side):
            position = lax.rem(seconds[half] + side - k, side)
            second_copy(half, k, p, position).wait_recv()
        total = second_in[half, 0, p].astype(F32)
        for position in range(1, side):
            total += second_in[half, position, p].astype(F32)
        target_of(half, firsts[half], p)[...] = total.astype(BF16)

    def exchange_send(half, p):
        for k in range(1, side):
            third_copy(half, k, p, firsts[half]).start()

    def finish_small():
        for c in range(n):
            total = small_buf[0, c]
            for source in range(1, chips):
                total += small_buf[source, c]
            total = sizes.scale * total
            cols = slice(c * w, (c + 1) * w)
            taps_out[:, cols] = taps_sum_ref[:, cols] + total[:count]
            bias_out[:, cols] = bias_sum_ref[:, cols] + total[count : count + 1]
        small_pair().wait_send()

    def drain_gather(d, carry):
        @pl.when(jnp.logical_and(d <= z, z < last))
        def _():
            line_sent(0, d).wait_send()

        @pl.when(jnp.logical_and(d >= z, z > 0))
        def _():
            line_sent(1, d).wait_send()

        return carry

    def drain_ring():
        for d in range(chips):
            if d > 0:

                @pl.when(d > z)
                def _():
                    ring_sent(0, d).wait_send()

            if d < last:

                @pl.when(d < z)
                def _():
                    ring_sent(1, d).wait_send()

    def each_kept(action):
        for skip, here in ((0, jnp.logical_not(skips)), (1, skips)):
            if skip == 0 or helped:

                @pl.when(here)
                def _():
                    for half in range(2):
                        for k in range(1, side):
                            action(half, k, skip)

    def drain_first():
        each_kept(lambda half, k, skip: first_sent(half, k, skip).wait_send())

    def drain_second():
        each_kept(lambda half, k, skip: second_sent(half, k, skip).wait_send())

    def drain_third(half, k, skip):
        shown = lax.rem(firsts[half] + side - k, side)
        third_done(half, k, shown, skip).wait_recv()
        third_done(half, k, firsts[half], skip).wait_send()

    def drain_early(j):
        @pl.when(j == rounds)
        def _():
            pair_sent().wait_send()
            lax.fori_loop(0, chips, drain_gather, 0)
            for c in range(max(n - 2, 0), n):
                term_copy(c).wait_send()

        @pl.when(j == 2 * rounds + 1)
        def _():
            drain_first()

    def drain_late():
        drain_second()
        finish_small()

    def send_own(c, carry):
        @pl.when(z < last)
        def _():
            line_copy(0, z, c).start()

        @pl.when(z > 0)
        def _():
            line_copy(1, z, c).start()

        pair_copy(z, c).start()
        return carry

    @pl.when(at_end)
    def _():
        lax.fori_loop(0, n, send_own, 0)

    def step(s, carry):
        i = s - far

        @pl.when(jnp.logical_and(s < n, jnp.logical_not(at_end)))
        def _():
            send_own(s, 0)

        for k in range(1, chips):
            c = s - k
            inside = jnp.logical_and(c >= 0, c < n)

            @pl.when(jnp.logical_and(inside, z - k >= 0))
            def _():
                arrive(0, z - k, c, z < last)

            @pl.when(jnp.logical_and(inside, z + k <= last))
            def _():
                arrive(1, z + k, c, z > 0)

        lax.fori_loop(termed(i - 1), termed(i), make_terms, 0)

        @pl.when(jnp.logical_and(i >= 0, i < n))
        def _():
            compute_first(i)

        lax.fori_loop(termed(i - 1), termed(i), wait_terms, 0)
        @pl.when(i == n)
        def _():
            send_small()

        turn = i - (n - 1) - 2 * rounds

        @pl.when(jnp.logical_and(turn >= 1, turn <= last))
        def _():
            pass_small(turn)

        lax.fori_loop(pushed(i - 1, z), pushed(i, z), push_up, 0)
        lax.fori_loop(pushed(i - 1, last - z), pushed(i, last - z), push_down, 0)
        hops = jnp.where(at_end, 2, far)
        lax.fori_loop(pushed(i - 2, hops), pushed(i - 1, hops), finish_sum, 0)

        drain_early(i - (n - 1))
        exchange(i - (n - 1))

        @pl.when(i == end)
        def _():
            drain_late()

        @pl.when(jnp.logical_and(i >= 0, i < n))
        def _():
            compute_second(i)

        @pl.when(jnp.logical_and(i >= n, i < 2 * n))
        def _():
            compute_later(i - n)

        return carry

    lax.fori_loop(0, end + last + 1, step, 0)

    drain_ring()

    def drain_small(o, carry):
        @pl.when(jnp.logical_and(o <= z, z < last))
        def _():
            small_copy(0, o).wait_send()

        @pl.when(jnp.logical_and(o >= z, z > 0))
        def _():
            small_copy(1, o).wait_send()

        return carry

    lax.fori_loop(0, chips, drain_small, 0)
    each_kept(drain_third)

    if helped:

        @pl.when(at_end)
        def _():
            help_copy().wait_send()
            back_done().wait_recv()

        @pl.when(helper)
        def _():
            back_done().wait_send()
            for half in range(2):
                for k in range(1, side):
                    first_copy(half, k, q).wait_send()
                    second_copy(half, k, q, seconds[half]).wait_send()
                    third_copy(half, k, q, firsts[half]).wait_send()


STORES = 4


def stores_of(rows):
    return STORES if rows % (16 * STORES) == 0 else 1


def store_kernel(*refs):
    count = len(refs) // 2
    sources, targets, sems = refs[:count], refs[count : 2 * count], refs[-1]
    copies = []
    for at in range(count):
        rows = sources[at].shape[0]
        parts = stores_of(rows)
        for part in range(parts):
            block = pl.ds(part * (rows // parts), rows // parts)
            copies.append(
                pltpu.make_async_copy(
                    sources[at].at[block], targets[at].at[block], sems.at[at, part]
                )
            )
    for copy in copies:
        copy.start()
    for copy in copies:
        copy.wait()


def on_device(
    rows_later,
    rows_earlier,
    out_cotangent,
    gate_proj,
    up_proj,
    conv_taps,
    conv_bias,
    gate_grad_sum,
    up_grad_sum,
    taps_grad_sum,
    bias_grad_sum,
):
    tokens, model = rows_later.shape
    depth, width = gate_proj.shape
    taps = conv_taps.shape[0]
    sizes = Sizes(
        lax.axis_size("fs"), lax.axis_size("tp"), tokens, model, depth, width, taps
    )
    n, w, q, r, cut = sizes.n, sizes.w, sizes.q, sizes.r, sizes.cut
    chips, side, fs_size = sizes.chips, sizes.side, sizes.fs_size
    dma = pltpu.SemaphoreType.DMA
    whole = pl.BlockSpec(memory_space=pltpu.VMEM)
    far = pl.BlockSpec(memory_space=pl.ANY)
    links = max(side - 1, 1)
    outs = pl.pallas_call(
        functools.partial(kernel, sizes),
        out_shape=(
            pltpu.VMEM((tokens, width), BF16),
            pltpu.VMEM((tokens, model), BF16),
            pltpu.VMEM((depth, width), F32),
            pltpu.VMEM((depth, width), F32),
            pltpu.VMEM((taps, width), F32),
            pltpu.VMEM((1, width), F32),
        ),
        in_specs=[far] * 11,
        out_specs=(whole,) * 6,
        scratch_shapes=[
            pltpu.VMEM((tokens, model), BF16),
            pltpu.VMEM((tokens, model), BF16),
            pltpu.VMEM((model, tokens), BF16),
            pltpu.VMEM((tokens, width), BF16),
            pltpu.VMEM((n, model, 2 * w), BF16),
            pltpu.VMEM((tokens, 2 * w), BF16),
            pltpu.VMEM((n, tokens, 2 * w), BF16),
            pltpu.VMEM((tokens, model), F32),
            pltpu.VMEM((n, chips * depth, 2 * w), BF16),
            pltpu.VMEM((2, chips * depth, 2 * w), BF16),
            pltpu.VMEM((n, chips * depth, 2 * w), BF16),
            pltpu.VMEM((2, n, max(chips - 1, 1), depth, 2 * w), BF16),
            pltpu.VMEM((tokens, model), BF16),
            pltpu.VMEM((tokens, cut), BF16),
            pltpu.VMEM((tokens, cut), BF16),
            dma((1,)),
            dma((1,)),
            dma((1,)),
            dma((1,)),
            pltpu.VMEM((2, links, q + 1, r, cut), BF16),
            pltpu.VMEM((2, side, q + 1, r, cut), BF16),
            pltpu.VMEM((n, 8 * -(-(taps + 1) // 8), w), F32),
            pltpu.VMEM((n, 8 * -(-(taps + 1) // 8), w), F32),
            pltpu.VMEM((chips, n, 8 * -(-(taps + 1) // 8), w), F32),
            pltpu.VMEM((taps, width), F32),
            pltpu.VMEM((1, width), F32),
            pltpu.VMEM((taps, width), F32),
            pltpu.VMEM((1, width), F32),
            dma((4,)),
            dma((2,)),
            dma((2,)),
            dma((1,)),
            dma((2,)),
            dma((2, chips)),
            dma((n, chips + 2)),
            dma((1,)),
            dma((n,)),
            dma((2,)),
            dma((n,)),
            dma((2, max(chips - 1, 1))),
            dma((2, links, 2)),
            dma((2, links, q + 1)),
            dma((2, links, 2)),
            dma((2, links, q + 1)),
            dma((2, links, 2)),
            dma((2, links, 2)),
            dma((3, chips)),
            dma((chips,)),
        ],
        compiler_params=pltpu.CompilerParams(
            collective_id=0, has_side_effects=True, vmem_limit_bytes=VMEM_BYTES
        ),
    )(
        rows_later,
        rows_earlier,
        out_cotangent,
        gate_proj,
        up_proj,
        gate_grad_sum,
        up_grad_sum,
        conv_taps,
        conv_bias[None],
        taps_grad_sum,
        bias_grad_sum[None],
    )
    stored = pl.pallas_call(
        store_kernel,
        out_shape=tuple(jax.ShapeDtypeStruct(out.shape, out.dtype) for out in outs),
        in_specs=[whole] * len(outs),
        out_specs=(far,) * len(outs),
        scratch_shapes=[dma((len(outs), STORES))],
        compiler_params=pltpu.CompilerParams(vmem_limit_bytes=1024 * 1024),
    )(*[pltpu.with_memory_space_constraint(out, pltpu.VMEM) for out in outs])
    return stored[:5] + (stored[5][0],)


def solution(mesh):
    placed = (
        P("fs", None),
        P("fs", None),
        P("fs", "tp"),
        P("fs", "tp"),
        P("fs", "tp"),
        P(None, "tp"),
        P("tp"),
        P("fs", "tp"),
        P("fs", "tp"),
        P(None, "tp"),
        P("tp"),
    )
    return jax.shard_map(
        on_device,
        mesh=mesh,
        in_specs=placed,
        out_specs=(
            P("fs", "tp"),
            P("fs", None),
            P("fs", "tp"),
            P("fs", "tp"),
            P(None, "tp"),
            P("tp"),
        ),
        check_vma=False,
    )
```

```python
import functools
import math

import jax
import jax.numpy as jnp
from jax import lax
from jax.experimental import pallas as pl
from jax.experimental.pallas import tpu as pltpu
from jax.sharding import PartitionSpec as P

MESH = pl.DeviceIdType.MESH
VMEM_BYTES = 57 * 1024 * 1024
FORWARD_ROWS = 768
F32, BF16 = jnp.float32, jnp.bfloat16


def contract_last(left, right):
    return lax.dot_general(
        left, right, (((1,), (1,)), ((), ())), preferred_element_type=jnp.float32
    )


def down(values, distance):
    if distance == 0:
        return values
    index = lax.broadcasted_iota(jnp.int32, values.shape, 0)
    return jnp.where(index >= distance, pltpu.roll(values, distance, 0), 0.0)


def up(values, distance):
    if distance == 0:
        return values
    rows = values.shape[0]
    index = lax.broadcasted_iota(jnp.int32, values.shape, 0)
    return jnp.where(index < rows - distance, pltpu.roll(values, rows - distance, 0), 0.0)


class Sizes:
    def __init__(self, fs_size, tp_size, tokens, model, depth, width, taps):
        self.fs_size = fs_size
        self.chips = fs_size // 2
        self.side = math.isqrt(tp_size)
        self.tokens, self.model, self.depth, self.width = tokens, model, depth, width
        self.w = math.gcd(width, 128)
        self.n = width // self.w
        self.taps = taps
        self.group = math.gcd(self.n, 2)
        self.tail = min(self.n, 2 * self.group)
        self.lead = min(self.n, 1)
        self.r = tokens // (2 * self.side)
        self.q = max(q for q in (1, 2, 4, 8) if model % (128 * q) == 0)
        self.cut = model // self.q
        self.scale = 1.0 / math.sqrt(tokens * fs_size)


def kernel(
    sizes,
    later_hbm,
    earlier_hbm,
    cot_hbm,
    gate_hbm,
    up_hbm,
    gate_sum_hbm,
    up_sum_hbm,
    taps_hbm,
    bias_hbm,
    taps_sum_hbm,
    bias_sum_hbm,
    hidden_out,
    rows_out,
    gate_out,
    up_out,
    taps_out,
    bias_out,
    later_v,
    earlier_v,
    earlier_t,
    cot_v,
    weights,
    pre,
    grads,
    acc,
    own_t,
    out_t,
    pair_t,
    ring,
    rows_s,
    help_in,
    help_out,
    help_send,
    help_recv,
    back_send,
    back_recv,
    first_in,
    second_in,
    small_v,
    small_in,
    small_buf,
    taps_ref,
    bias_ref,
    taps_sum_ref,
    bias_sum_ref,
    mix_load,
    weight_load,
    rows_load,
    cot_load,
    sum_load,
    line_send,
    line_recv,
    pair_send,
    pair_recv,
    term_send,
    term_recv,
    ring_send,
    first_send,
    first_recv,
    second_send,
    second_recv,
    third_send,
    third_recv,
    small_send,
    small_recv,
):
    n, w, q, r, cut = sizes.n, sizes.w, sizes.q, sizes.r, sizes.cut
    group, tail, lead = sizes.group, sizes.tail, sizes.lead
    chips, side, depth = sizes.chips, sizes.side, sizes.depth
    fs_size, tokens, model = sizes.fs_size, sizes.tokens, sizes.model
    count = sizes.taps
    last = chips - 1
    fs = lax.axis_index("fs")
    tp = lax.axis_index("tp")
    z = fs // 2
    core = lax.rem(fs, 2)
    partner = 2 * z + 1 - core
    at_end = jnp.logical_or(z == 0, z == last)
    helped = chips >= 4
    helper = jnp.logical_and(helped, jnp.logical_or(z == 1, z == last - 1))
    neighbours = (lax.rem(fs + 2, fs_size), lax.rem(fs + fs_size - 2, fs_size))
    ty = tp // side
    tx = lax.rem(tp, side)
    firsts = (tx, ty)
    seconds = (ty, tx)

    def first_peer(half, k):
        peer = lax.rem(firsts[half] + k, side)
        return peer, (ty * side + peer if half == 0 else peer * side + tx)

    def second_peer(half, k):
        peer = lax.rem(seconds[half] + k, side)
        return peer, (peer * side + tx if half == 0 else ty * side + peer)

    def columns(c):
        return pl.ds(pl.multiple_of(c * w, w), w)

    def own_rows(which):
        return pl.ds(pl.multiple_of((2 * z + which) * depth, depth), depth)

    def load_weight(c, which):
        source = (gate_hbm, up_hbm)[which]
        return pltpu.make_async_copy(
            source.at[:, columns(c)],
            weights.at[c, own_rows(core), pl.ds(which * w, w)],
            weight_load.at[which],
        )

    def wait_weights():
        for which in range(2):
            ref = weights.at[:, own_rows(core), pl.ds(which * w, w)]
            pltpu.make_async_copy(ref, ref, weight_load.at[which]).wait()

    def load_rows(which):
        return pltpu.make_async_copy(
            (later_hbm, earlier_hbm)[which], (later_v, earlier_v)[which], rows_load.at[which]
        )

    def load_cot():
        return pltpu.make_async_copy(cot_hbm, cot_v, cot_load.at[0])

    def load_mix(which):
        sources = (taps_hbm, bias_hbm, taps_sum_hbm, bias_sum_hbm)
        targets = (taps_ref, bias_ref, taps_sum_ref, bias_sum_ref)
        return pltpu.make_async_copy(sources[which], targets[which], mix_load.at[which])

    def load_sum(which):
        return pltpu.make_async_copy(
            (gate_sum_hbm, up_sum_hbm)[which], (gate_out, up_out)[which], sum_load.at[which]
        )

    def block_of(half, i):
        return pl.ds(pl.multiple_of((half * side + i) * r, r), r)

    def piece(half, i, p):
        return block_of(half, i), pl.ds(pl.multiple_of(p * cut, cut), cut)

    def remote(source, target, send, recv, device):
        return pltpu.make_async_remote_copy(
            src_ref=source,
            dst_ref=target,
            send_sem=send,
            recv_sem=recv,
            device_id=device,
            device_id_type=MESH,
        )

    def shard(o, which, c):
        return weights.at[c, pl.ds(pl.multiple_of((2 * o + which) * depth, depth), depth)]

    def line_copy(way, o, c):
        ref = shard(o, core, c)
        return remote(
            ref, ref, line_send.at[way, o], line_recv.at[c, o], {"fs": neighbours[way]}
        )

    def line_sent(way, o):
        rows = pl.ds(pl.multiple_of((2 * o + core) * depth, depth), depth)
        ref = weights.at[:, rows]
        return remote(
            ref, ref, line_send.at[way, o], line_recv.at[0, 0], {"fs": neighbours[way]}
        )

    def pair_copy(o, c):
        ref = shard(o, core, c)
        return remote(ref, ref, pair_send.at[0], pair_recv.at[c], {"fs": partner})

    def pair_received(c):
        ref = weights.at[c, pl.ds(0, chips * depth)]
        return remote(ref, ref, pair_send.at[0], pair_recv.at[c], {"fs": partner})

    def pair_sent():
        ref = weights.at[:, pl.ds(0, chips * depth)]
        return remote(ref, ref, pair_send.at[0], pair_recv.at[0], {"fs": partner})

    def term_copy(c):
        return remote(
            out_t.at[lax.rem(c, 2)],
            pair_t.at[c],
            term_send.at[lax.rem(c, 2)],
            term_recv.at[c],
            {"fs": partner},
        )

    def ring_slot(way, c, d):
        return ring.at[way, c, d - 1 if way == 0 else d]

    def ring_copy(way, c, d, at):
        index = d - 1 if way == 0 else d
        recv = line_recv.at[c, jnp.where(d == at, chips + way, d)]
        slot = ring.at[way, c, index]
        return remote(
            slot,
            slot,
            ring_send.at[way, index],
            recv,
            {"fs": neighbours[way]},
        )

    def ring_sent(way, d):
        index = d - 1 if way == 0 else d
        ref = ring.at[way, :, index]
        return remote(
            ref, ref, ring_send.at[way, index], line_recv.at[0, 0], {"fs": neighbours[way]}
        )

    def extra(p):
        return int(isinstance(p, int) and p == q)

    def source_of(half, i, p):
        if isinstance(p, int) and p == q:
            return help_in.at[block_of(half, i)]
        return rows_s.at[piece(half, i, p)]

    def target_of(half, i, p):
        if isinstance(p, int) and p == q:
            return help_out.at[block_of(half, i)]
        return rows_out.at[piece(half, i, p)]

    def first_copy(half, k, p):
        peer, device = first_peer(half, k)
        at = (half, k - 1, p)
        return remote(
            source_of(half, peer, p),
            first_in.at[at],
            first_send.at[half, k - 1, extra(p)],
            first_recv.at[at],
            {"tp": device},
        )

    def second_copy(half, k, p, position):
        _, device = second_peer(half, k)
        slot = second_in.at[half, position, p]
        at = (half, k - 1, p)
        return remote(
            slot, slot, second_send.at[half, k - 1, extra(p)], second_recv.at[at], {"tp": device}
        )

    def third_copy(half, k, p, shown):
        _, device = first_peer(half, k)
        ref = target_of(half, shown, p)
        at = (half, k - 1, extra(p))
        return remote(ref, ref, third_send.at[at], third_recv.at[at], {"tp": device})

    def first_sent(half, k, skip):
        peer, device = first_peer(half, k)
        ref = rows_s.at[block_of(half, peer), pl.ds(skip * cut, model - skip * cut)]
        at = (half, k - 1, 0)
        return remote(ref, ref, first_send.at[at], first_recv.at[at], {"tp": device})

    def second_sent(half, k, skip):
        _, device = second_peer(half, k)
        ref = second_in.at[half, seconds[half], pl.ds(skip, q - skip)]
        at = (half, k - 1, 0)
        return remote(ref, ref, second_send.at[at], second_recv.at[at], {"tp": device})

    def third_done(half, k, shown, skip):
        _, device = first_peer(half, k)
        ref = rows_out.at[block_of(half, shown), pl.ds(skip * cut, model - skip * cut)]
        at = (half, k - 1, 0)
        return remote(ref, ref, third_send.at[at], third_recv.at[at], {"tp": device})

    def help_copy():
        device = jnp.where(z == 0, neighbours[0], neighbours[1])
        source = rows_s.at[:, pl.ds(0, cut)]
        return remote(source, help_in, help_send.at[0], help_recv.at[0], {"fs": device})

    def back_copy(half, i):
        device = jnp.where(z == 1, neighbours[1], neighbours[0])
        return remote(
            help_out.at[block_of(half, i)],
            rows_out.at[piece(half, i, 0)],
            back_send.at[0],
            back_recv.at[0],
            {"fs": device},
        )

    def back_done():
        device = jnp.where(z == 1, neighbours[1], neighbours[0])
        target = rows_out.at[:, pl.ds(0, cut)]
        return remote(help_out, target, back_send.at[0], back_recv.at[0], {"fs": device})

    def small_pair():
        return remote(small_v, small_in, small_send.at[2, 0], small_recv.at[z], {"fs": partner})

    def small_copy(way, o):
        ref = small_buf.at[o]
        return remote(
            ref, ref, small_send.at[way, o], small_recv.at[o], {"fs": neighbours[way]}
        )

    def send_small():
        small_pair().wait_recv()
        low = jnp.where(core == 0, small_v[...], small_in[...])
        high = jnp.where(core == 0, small_in[...], small_v[...])
        small_buf[z] = low + high

        @pl.when(z < last)
        def _():
            small_copy(0, z).start()

        @pl.when(z > 0)
        def _():
            small_copy(1, z).start()

    def pass_small(k):
        @pl.when(z - k >= 0)
        def _():
            small_copy(0, z - k).wait_recv()

            @pl.when(z < last)
            def _():
                small_copy(0, z - k).start()

        @pl.when(z + k <= last)
        def _():
            small_copy(1, z + k).wait_recv()

            @pl.when(z > 0)
            def _():
                small_copy(1, z + k).start()

    for c in range(n):
        load_weight(c, 0).start()
        load_weight(c, 1).start()

    barrier = pltpu.get_barrier_semaphore()
    def greet(device):
        pl.semaphore_signal(barrier, inc=1, device_id={"fs": device}, device_id_type=MESH)

    @pl.when(z < last)
    def _():
        greet(neighbours[0])

    @pl.when(z > 0)
    def _():
        greet(neighbours[1])

    greet(partner)
    for half in range(2):
        for k in range(1, side):
            pl.semaphore_signal(
                barrier, inc=1, device_id={"tp": first_peer(half, k)[1]}, device_id_type=MESH
            )

    load_rows(1).start()
    load_cot().start()
    load_rows(0).start()
    for which in range(4):
        load_mix(which).start()
    load_sum(0).start()
    load_sum(1).start()

    expected = 1 + 2 * (side - 1) + jnp.where(z < last, 1, 0) + jnp.where(z > 0, 1, 0)
    pl.semaphore_wait(barrier, expected)
    wait_weights()

    block = math.gcd(tokens, FORWARD_ROWS)

    def forward(rows_v, c):
        def body(index, carry):
            rows = pl.ds(pl.multiple_of(index * block, block), block)
            value = jnp.dot(rows_v[rows, :], weights[c], preferred_element_type=F32)
            pre[rows, :] = value.astype(BF16)
            return carry

        lax.fori_loop(0, tokens // block, body, 0)

    def mixing(c):
        gate = pre[:, :w].astype(F32)
        value = pre[:, w:].astype(F32)
        taps = [taps_ref[k : k + 1, columns(c)] for k in range(count)]
        shifted = [down(gate, count - 1 - k) for k in range(count)]
        mixed = bias_ref[:, columns(c)] + taps[0] * shifted[0]
        for k in range(1, count):
            mixed += taps[k] * shifted[k]
        sig = jax.nn.sigmoid(mixed)
        return value, taps, shifted, mixed, sig

    def middle_later(c):
        value, _, _, mixed, sig = mixing(c)
        hidden_out[:, columns(c)] = (mixed * sig * value).astype(BF16)

    def middle_earlier(c):
        value, taps, shifted, mixed, sig = mixing(c)
        cot = cot_v[:, columns(c)].astype(F32)
        grads[c, :, w:] = (cot * (mixed * sig)).astype(BF16)
        mixed_grad = cot * value * sig * (1.0 + mixed * (1.0 - sig))
        total = taps[count - 1] * mixed_grad
        for k in range(count - 1):
            total += taps[k] * up(mixed_grad, count - 1 - k)
        grads[c, :, :w] = total.astype(BF16)
        for k in range(count):
            small_v[c, k : k + 1, :] = jnp.sum(mixed_grad * shifted[k], axis=0, keepdims=True)
        small_v[c, count : count + 1, :] = jnp.sum(mixed_grad, axis=0, keepdims=True)

    def rows_part(c, chunks, cols):
        value = contract_last(grads[c - chunks + 1], weights[c - chunks + 1, cols, :])
        for k in range(1, chunks):
            at = c - chunks + 1 + k
            value += contract_last(grads[at], weights[at, cols, :])
        return value

    def add_rows(c):
        wide = math.gcd(model, 512)

        def body(p, carry):
            cols = pl.ds(pl.multiple_of(p * wide, wide), wide)
            acc[:, cols] += rows_part(c, group, cols)
            return carry

        lax.fori_loop(0, model // wide, body, 0)

    skips = jnp.logical_and(helped, at_end)

    def kept(p):
        return jnp.logical_not(jnp.logical_and(skips, p == 0))

    def start_first(p):
        @pl.when(kept(p))
        def _():
            for k in range(1, side):
                for half in range(2):
                    first_copy(half, k, p).start()

        @pl.when(jnp.logical_not(kept(p)))
        def _():
            help_copy().start()

    def last_rows(c):
        late = q // 2

        def body(turn, carry):
            moved = jnp.where(turn < late, turn + 1, jnp.where(turn == late, 0, turn))
            p = jnp.where(skips, moved, turn)
            cols = pl.ds(pl.multiple_of(p * cut, cut), cut)
            rows_s[:, cols] = (acc[:, cols] + rows_part(c, tail, cols)).astype(BF16)
            start_first(p)
            return carry

        lax.fori_loop(0, q, body, 0)

    def make_terms(c, carry):
        slot = lax.rem(c, 2)

        @pl.when(c >= 2)
        def _():
            term_copy(c - 2).wait_send()

        half_rows = chips * depth
        value = jnp.dot(earlier_t[...], grads[c], preferred_element_type=F32)
        out_t[slot] = value[:half_rows].astype(BF16)
        own_t[c] = value[half_rows:].astype(BF16)
        term_copy(c).start()
        return carry

    def wait_terms(c, carry):
        term_copy(c).wait_recv()
        return carry

    def transpose_rows():
        acc[...] = jnp.zeros_like(acc)
        small_v[...] = jnp.zeros_like(small_v)

        def body(d, carry):
            cols = pl.ds(pl.multiple_of(d * 2 * depth, 2 * depth), 2 * depth)
            value = earlier_v[:, cols].T
            for which in range(2):
                owner = jnp.where(core == which, chips + d, d)
                rows = pl.ds(pl.multiple_of(owner * depth, depth), depth)
                earlier_t[rows, :] = value[which * depth : (which + 1) * depth]
            return carry

        lax.fori_loop(0, chips, body, 0)

    def compute_first(c):
        @pl.when(c == 0)
        def _():
            load_rows(1).wait()
            load_cot().wait()
            for which in range(4):
                load_mix(which).wait()
            load_sum(0).wait()
            load_sum(1).wait()
            transpose_rows()

        pair_received(c).wait_recv()
        forward(earlier_v, c)

    def compute_second(c):
        middle_earlier(c)
        lax.fori_loop(made(c - 1), jnp.where(c < n - 1, made(c), made(c - 1)), make_terms, 0)

        @pl.when(jnp.logical_and(c < n - tail, lax.rem(c, group) == group - 1))
        def _():
            add_rows(c)

        @pl.when(c == n - 1)
        def _():
            last_rows(c)
            small_pair().start()

    def compute_later(c):
        @pl.when(c == 0)
        def _():
            load_rows(0).wait()

        forward(later_v, c)
        middle_later(c)

    def arrive(way, o, c, goes_on):
        line_copy(way, o, c).wait_recv()

        @pl.when(goes_on)
        def _():
            line_copy(way, o, c).start()

        pair_copy(o, c).start()

    def terms_of(c, d):
        rows = pl.ds(pl.multiple_of(d * depth, depth), depth)
        return own_t[c, rows, :].astype(F32) + pair_t[c, rows, :].astype(F32)

    def push(way, c, d, first_on_line):
        slot = ring_slot(way, c, d)

        @pl.when(first_on_line)
        def _():
            slot[...] = terms_of(c, d).astype(BF16)

        @pl.when(jnp.logical_not(first_on_line))
        def _():
            ring_copy(way, c, d, z).wait_recv()
            slot[...] = (terms_of(c, d) + slot[...].astype(F32)).astype(BF16)

        ring_copy(way, c, d, z + 1 if way == 0 else z - 1).start()

    def push_up(c, carry):
        for d in range(last, 0, -1):

            @pl.when(d > z)
            def _():
                push(0, c, d, z == 0)

        return carry

    def push_down(c, carry):
        for d in range(last):

            @pl.when(d < z)
            def _():
                push(1, c, d, z == last)

        return carry

    def finish_sum(c, carry):
        def add(value):
            gate_out[:, columns(c)] += sizes.scale * value[:, :w]
            up_out[:, columns(c)] += sizes.scale * value[:, w:]

        base = terms_of(c, z)

        @pl.when(z == 0)
        def _():
            ring_copy(1, c, z, z).wait_recv()
            add(base + ring_slot(1, c, z)[...].astype(F32))

        @pl.when(z == last)
        def _():
            ring_copy(0, c, z, z).wait_recv()
            add(base + ring_slot(0, c, z)[...].astype(F32))

        @pl.when(jnp.logical_and(z > 0, z < last))
        def _():
            ring_copy(0, c, z, z).wait_recv()
            ring_copy(1, c, z, z).wait_recv()
            add(
                base
                + ring_slot(0, c, z)[...].astype(F32)
                + ring_slot(1, c, z)[...].astype(F32)
            )

        return carry

    far = jnp.maximum(z, last - z)

    def termed(i):
        return jnp.where(i >= n, n, jnp.clip(i, 0, max(n - 2, 0)))

    def made(i):
        return jnp.where(i >= n, n, jnp.clip(i + 1, 0, max(n - 2, 0)))

    def pushed(i, hops):
        turn = i - (n - 1)
        near = jnp.maximum(jnp.minimum(3 + (turn - 1) // 2, n - 2), turn - 3)
        near = jnp.where(turn >= 1, near, 0)
        turn -= 2 * (hops - 2)
        distant = jnp.maximum(jnp.minimum(turn - 3, n - 2), turn - 4)
        after = jnp.clip(jnp.where(hops == 1, near, distant), 0, n)
        return jnp.where(hops == 0, termed(i), after)

    batch = math.gcd(q, 2)
    rounds = q // batch

    hold = jnp.where(helper, rounds - 1, 0)
    turns = max(n + 5, n - 1 + 2 * last, 2 * rounds + last + 1, 3 * rounds, 2 * rounds + 3)
    end = n - 1 + turns

    def exchange(j):
        def during(first, action):
            @pl.when(jnp.logical_and(j > first, j <= first + rounds))
            def _():
                for at in range(batch):
                    p = (j - 1 - first) * batch + at

                    @pl.when(kept(p))
                    def _():
                        for half in range(2):
                            action(half, p)

        during(0, exchange_first)
        during(rounds, exchange_second)
        if helped:
            assist(j - 2 * rounds)
        during(rounds + hold, exchange_send)

    def assist(turn):
        @pl.when(jnp.logical_and(helper, turn == 0))
        def _():
            help_copy().wait_recv()
            for k in range(1, side):
                for half in range(2):
                    first_copy(half, k, q).start()

        @pl.when(jnp.logical_and(helper, turn == 1))
        def _():
            for half in range(2):
                exchange_first(half, q)

        @pl.when(jnp.logical_and(helper, turn == 2))
        def _():
            for half in range(2):
                exchange_second(half, q)
                exchange_send(half, q)
                back_copy(half, firsts[half]).start()

        @pl.when(jnp.logical_and(helper, turn == 3))
        def _():
            for half in range(2):
                for k in range(1, side):
                    shown = lax.rem(firsts[half] + side - k, side)
                    third_copy(half, k, q, shown).wait_recv()
                    back_copy(half, shown).start()

    def exchange_first(half, p):
        total = source_of(half, firsts[half], p)[...].astype(F32)
        for k in range(1, side):
            first_copy(half, k, p).wait_recv()
            total += first_in[half, k - 1, p].astype(F32)
        second_in[half, seconds[half], p] = total.astype(BF16)
        for k in range(1, side):
            second_copy(half, k, p, seconds[half]).start()

    def exchange_second(half, p):
        for k in range(1, side):
            position = lax.rem(seconds[half] + side - k, side)
            second_copy(half, k, p, position).wait_recv()
        total = second_in[half, 0, p].astype(F32)
        for position in range(1, side):
            total += second_in[half, position, p].astype(F32)
        target_of(half, firsts[half], p)[...] = total.astype(BF16)

    def exchange_send(half, p):
        for k in range(1, side):
            third_copy(half, k, p, firsts[half]).start()

    def finish_small():
        for c in range(n):
            total = small_buf[0, c]
            for source in range(1, chips):
                total += small_buf[source, c]
            total = sizes.scale * total
            cols = slice(c * w, (c + 1) * w)
            taps_out[:, cols] = taps_sum_ref[:, cols] + total[:count]
            bias_out[:, cols] = bias_sum_ref[:, cols] + total[count : count + 1]
        small_pair().wait_send()

    def drain_gather(d, carry):
        @pl.when(jnp.logical_and(d <= z, z < last))
        def _():
            line_sent(0, d).wait_send()

        @pl.when(jnp.logical_and(d >= z, z > 0))
        def _():
            line_sent(1, d).wait_send()

        return carry

    def drain_ring():
        for d in range(chips):
            if d > 0:

                @pl.when(d > z)
                def _():
                    ring_sent(0, d).wait_send()

            if d < last:

                @pl.when(d < z)
                def _():
                    ring_sent(1, d).wait_send()

    def each_kept(action):
        for skip, here in ((0, jnp.logical_not(skips)), (1, skips)):
            if skip == 0 or helped:

                @pl.when(here)
                def _():
                    for half in range(2):
                        for k in range(1, side):
                            action(half, k, skip)

    def drain_first():
        each_kept(lambda half, k, skip: first_sent(half, k, skip).wait_send())

    def drain_second():
        each_kept(lambda half, k, skip: second_sent(half, k, skip).wait_send())

    def drain_third(half, k, skip):
        shown = lax.rem(firsts[half] + side - k, side)
        third_done(half, k, shown, skip).wait_recv()
        third_done(half, k, firsts[half], skip).wait_send()

    def drain_early(j):
        @pl.when(j == rounds)
        def _():
            pair_sent().wait_send()
            lax.fori_loop(0, chips, drain_gather, 0)
            for c in range(max(n - 2, 0), n):
                term_copy(c).wait_send()

        @pl.when(j == 2 * rounds + 1)
        def _():
            drain_first()

    def drain_late():
        drain_second()
        finish_small()

    heavy = jnp.where(2 * z < last, 1, 0)

    def send_heavy(c):
        for way, goes_on in ((0, z < last), (1, z > 0)):

            @pl.when(jnp.logical_and(heavy == way, goes_on))
            def _():
                line_copy(way, z, c).start()

    def send_light(c):
        for way, goes_on in ((0, z < last), (1, z > 0)):

            @pl.when(jnp.logical_and(heavy != way, goes_on))
            def _():
                line_copy(way, z, c).start()

        pair_copy(z, c).start()

    def send_all(c, carry):
        send_heavy(c)
        send_light(c)
        return carry

    @pl.when(at_end)
    def _():
        lax.fori_loop(0, n, send_all, 0)

    @pl.when(jnp.logical_not(at_end))
    def _():
        for c in range(lead):
            send_heavy(c)

    def step(s, carry):
        i = s - far

        @pl.when(jnp.logical_and(s + lead < n, jnp.logical_not(at_end)))
        def _():
            send_heavy(s + lead)

        @pl.when(jnp.logical_and(s < n, jnp.logical_not(at_end)))
        def _():
            send_light(s)

        @pl.when(i == n)
        def _():
            lax.fori_loop(made(n - 1), n, make_terms, 0)

        early = jnp.logical_or(at_end, i >= n)
        lax.fori_loop(termed(i - 1), jnp.where(early, termed(i), termed(i - 1)), wait_terms, 0)
        @pl.when(i == n)
        def _():
            send_small()

        turn = i - (n - 1) - 2 * rounds

        @pl.when(jnp.logical_and(turn >= 1, turn <= last))
        def _():
            pass_small(turn)

        lax.fori_loop(pushed(i - 1, z), pushed(i, z), push_up, 0)
        lax.fori_loop(pushed(i - 1, last - z), pushed(i, last - z), push_down, 0)
        hops = jnp.where(at_end, 2, far)
        lax.fori_loop(pushed(i - 2, hops), pushed(i - 1, hops), finish_sum, 0)

        for k in range(1, chips):
            c = s - k
            inside = jnp.logical_and(c >= 0, c < n)

            @pl.when(jnp.logical_and(inside, z - k >= 0))
            def _():
                arrive(0, z - k, c, z < last)

            @pl.when(jnp.logical_and(inside, z + k <= last))
            def _():
                arrive(1, z + k, c, z > 0)

        @pl.when(jnp.logical_and(i >= 0, i < n))
        def _():
            compute_first(i)

        lax.fori_loop(jnp.where(early, termed(i), termed(i - 1)), termed(i), wait_terms, 0)
        drain_early(i - (n - 1))
        exchange(i - (n - 1))

        @pl.when(i == end)
        def _():
            drain_late()

        @pl.when(jnp.logical_and(i >= 0, i < n))
        def _():
            compute_second(i)

        @pl.when(jnp.logical_and(i >= n, i < 2 * n))
        def _():
            compute_later(i - n)

        return carry

    lax.fori_loop(0, end + last + 1, step, 0)

    drain_ring()

    def drain_small(o, carry):
        @pl.when(jnp.logical_and(o <= z, z < last))
        def _():
            small_copy(0, o).wait_send()

        @pl.when(jnp.logical_and(o >= z, z > 0))
        def _():
            small_copy(1, o).wait_send()

        return carry

    lax.fori_loop(0, chips, drain_small, 0)
    each_kept(drain_third)

    if helped:

        @pl.when(at_end)
        def _():
            help_copy().wait_send()
            back_done().wait_recv()

        @pl.when(helper)
        def _():
            back_done().wait_send()
            for half in range(2):
                for k in range(1, side):
                    first_copy(half, k, q).wait_send()
                    second_copy(half, k, q, seconds[half]).wait_send()
                    third_copy(half, k, q, firsts[half]).wait_send()


STORES = 4


def stores_of(rows):
    return STORES if rows % (16 * STORES) == 0 else 1


def store_kernel(*refs):
    count = len(refs) // 2
    sources, targets, sems = refs[:count], refs[count : 2 * count], refs[-1]
    copies = []
    for at in range(count):
        rows = sources[at].shape[0]
        parts = stores_of(rows)
        for part in range(parts):
            block = pl.ds(part * (rows // parts), rows // parts)
            copies.append(
                pltpu.make_async_copy(
                    sources[at].at[block], targets[at].at[block], sems.at[at, part]
                )
            )
    for copy in copies:
        copy.start()
    for copy in copies:
        copy.wait()


def on_device(
    rows_later,
    rows_earlier,
    out_cotangent,
    gate_proj,
    up_proj,
    conv_taps,
    conv_bias,
    gate_grad_sum,
    up_grad_sum,
    taps_grad_sum,
    bias_grad_sum,
):
    tokens, model = rows_later.shape
    depth, width = gate_proj.shape
    taps = conv_taps.shape[0]
    sizes = Sizes(
        lax.axis_size("fs"), lax.axis_size("tp"), tokens, model, depth, width, taps
    )
    n, w, q, r, cut = sizes.n, sizes.w, sizes.q, sizes.r, sizes.cut
    chips, side, fs_size = sizes.chips, sizes.side, sizes.fs_size
    dma = pltpu.SemaphoreType.DMA
    whole = pl.BlockSpec(memory_space=pltpu.VMEM)
    far = pl.BlockSpec(memory_space=pl.ANY)
    links = max(side - 1, 1)
    outs = pl.pallas_call(
        functools.partial(kernel, sizes),
        out_shape=(
            pltpu.VMEM((tokens, width), BF16),
            pltpu.VMEM((tokens, model), BF16),
            pltpu.VMEM((depth, width), F32),
            pltpu.VMEM((depth, width), F32),
            pltpu.VMEM((taps, width), F32),
            pltpu.VMEM((1, width), F32),
        ),
        in_specs=[far] * 11,
        out_specs=(whole,) * 6,
        scratch_shapes=[
            pltpu.VMEM((tokens, model), BF16),
            pltpu.VMEM((tokens, model), BF16),
            pltpu.VMEM((model, tokens), BF16),
            pltpu.VMEM((tokens, width), BF16),
            pltpu.VMEM((n, model, 2 * w), BF16),
            pltpu.VMEM((tokens, 2 * w), BF16),
            pltpu.VMEM((n, tokens, 2 * w), BF16),
            pltpu.VMEM((tokens, model), F32),
            pltpu.VMEM((n, chips * depth, 2 * w), BF16),
            pltpu.VMEM((2, chips * depth, 2 * w), BF16),
            pltpu.VMEM((n, chips * depth, 2 * w), BF16),
            pltpu.VMEM((2, n, max(chips - 1, 1), depth, 2 * w), BF16),
            pltpu.VMEM((tokens, model), BF16),
            pltpu.VMEM((tokens, cut), BF16),
            pltpu.VMEM((tokens, cut), BF16),
            dma((1,)),
            dma((1,)),
            dma((1,)),
            dma((1,)),
            pltpu.VMEM((2, links, q + 1, r, cut), BF16),
            pltpu.VMEM((2, side, q + 1, r, cut), BF16),
            pltpu.VMEM((n, 8 * -(-(taps + 1) // 8), w), F32),
            pltpu.VMEM((n, 8 * -(-(taps + 1) // 8), w), F32),
            pltpu.VMEM((chips, n, 8 * -(-(taps + 1) // 8), w), F32),
            pltpu.VMEM((taps, width), F32),
            pltpu.VMEM((1, width), F32),
            pltpu.VMEM((taps, width), F32),
            pltpu.VMEM((1, width), F32),
            dma((4,)),
            dma((2,)),
            dma((2,)),
            dma((1,)),
            dma((2,)),
            dma((2, chips)),
            dma((n, chips + 2)),
            dma((1,)),
            dma((n,)),
            dma((2,)),
            dma((n,)),
            dma((2, max(chips - 1, 1))),
            dma((2, links, 2)),
            dma((2, links, q + 1)),
            dma((2, links, 2)),
            dma((2, links, q + 1)),
            dma((2, links, 2)),
            dma((2, links, 2)),
            dma((3, chips)),
            dma((chips,)),
        ],
        compiler_params=pltpu.CompilerParams(
            collective_id=0, has_side_effects=True, vmem_limit_bytes=VMEM_BYTES
        ),
    )(
        rows_later,
        rows_earlier,
        out_cotangent,
        gate_proj,
        up_proj,
        gate_grad_sum,
        up_grad_sum,
        conv_taps,
        conv_bias[None],
        taps_grad_sum,
        bias_grad_sum[None],
    )
    stored = pl.pallas_call(
        store_kernel,
        out_shape=tuple(jax.ShapeDtypeStruct(out.shape, out.dtype) for out in outs),
        in_specs=[whole] * len(outs),
        out_specs=(far,) * len(outs),
        scratch_shapes=[dma((len(outs), STORES))],
        compiler_params=pltpu.CompilerParams(vmem_limit_bytes=1024 * 1024),
    )(*[pltpu.with_memory_space_constraint(out, pltpu.VMEM) for out in outs])
    return stored[:5] + (stored[5][0],)


def solution(mesh):
    placed = (
        P("fs", None),
        P("fs", None),
        P("fs", "tp"),
        P("fs", "tp"),
        P("fs", "tp"),
        P(None, "tp"),
        P("tp"),
        P("fs", "tp"),
        P("fs", "tp"),
        P(None, "tp"),
        P("tp"),
    )
    return jax.shard_map(
        on_device,
        mesh=mesh,
        in_specs=placed,
        out_specs=(
            P("fs", "tp"),
            P("fs", None),
            P("fs", "tp"),
            P("fs", "tp"),
            P(None, "tp"),
            P("tp"),
        ),
        check_vma=False,
    )
```
